32 devices in a mesh: sp: 8 (over z, x), tp: 4 (over y, core).
Axes of the slice: x: 2, y: 2, z: 4, core: 2. Of those that a mesh axis runs over, the one named last changes fastest.
Arguments:
- receptance: bfloat16 [1024, 1024], P('sp', 'tp'), may hold values from -6 to 6
- key_by_head: bfloat16 [1024, 1024], P('sp', 'tp'), may hold values from -6 to 6
- value_head_rows: bfloat16 [1024, 1024], P('sp', 'tp'), may hold values from -6 to 6
- decay_preact: bfloat16 [1024, 1024], P('sp', 'tp'), may hold values from -13 to -0.5
- correction_preact: bfloat16 [1024, 1024], P('sp', 'tp'), may hold values from -7 to 3
- result_sigmoid_factor: bfloat16 [1024, 1024], P('sp', 'tp'), may hold values from -6 to 6
- key_rate_mixing: float32 [1024], P('tp'), may hold values from 0.3 to 0.9
- diagonal_current_factor: float32 [1024], P('tp'), may hold values from -0.6 to 0.6
- per_head_gain: float32 [1024], P('tp'), may hold values from 0.1 to 1.9
- per_head_bias: float32 [1024], P('tp'), may hold values from -1.5 to 1.5
- output_matrix: bfloat16 [1024, 2048], P('tp'), may hold values from -0.1875 to 0.1875
- residual: bfloat16 [1024, 2048], P('sp'), may hold values from -6 to 6
- expert_norm_gain: float32 [2048], replicated, may hold values from 0.1 to 1.9
- routes: int32 [1024, 8], P('sp'), may hold values from 0 to 31, all different within a row; in each aligned block of 128 rows (0 to 127, 128 to 255, ...) at most 48 rows name the same one
- chosen_expert_weight: float32 [1024, 8], P('sp'), may hold values from 0.05 to 0.6
- routed_gate_weight: bfloat16 [32, 2048, 512], P(('sp', 'tp')), may hold values from -0.125 to 0.125
- routed_up_weight: bfloat16 [32, 2048, 512], P(('sp', 'tp')), may hold values from -0.125 to 0.125
- routed_down_weight: bfloat16 [32, 512, 2048], P(('sp', 'tp')), may hold values from -0.25 to 0.25
- common_gate_weight: bfloat16 [2048, 512], P(None, 'tp'), may hold values from -0.125 to 0.125
- common_up_weight: bfloat16 [2048, 512], P(None, 'tp'), may hold values from -0.125 to 0.125
- common_down_weight: bfloat16 [512, 2048], P('tp'), may hold values from -0.25 to 0.25
Outputs:
- layer_out: bfloat16 [1024, 2048], P('sp', 'tp')
The draws below stay inside these ranges and needn't reach their ends.
Inputs may be any that keep to these rules, and one draw needn't show every extreme that they name: `routes`: each row names 8 different experts; in each aligned block of 128 rows no expert is named by more than 48 rows.
All inputs are finite; a program needn't handle non-finite values.
Results may differ from the reference program's by a relative error of at most 0.018.
Values may be sent and summed in bfloat16 or wider, within the bound.
A program may use at most 64 MiB of HBM per device.

```python
import math
import jax
import jax.numpy as jnp
import numpy as np
from jax import lax

D = 2048
HEADS = 16
CHANNEL_SPAN = 64
FF = 512
TOP_K = 8
TOK_DEV = 128
INNER_WIDTH = 1024
EXPERTS = 32
TOKENS = 1024
CAP = 48
N_SP = 8


def head_pattern(key):
    chance = 0.5
    slow_heads = jax.random.bernoulli(jax.random.fold_in(key, 11), chance, (HEADS,))
    return jnp.repeat(slow_heads, CHANNEL_SPAN)


def draw_decay_preact(key, part):
    slow_cols = head_pattern(key)
    jitter = jax.random.uniform(jax.random.fold_in(key, 21), (TOKENS, INNER_WIDTH), jnp.float32, -1.5, 1.5)
    block_count = TOKENS // TOK_DEV
    offsets = jax.random.uniform(jax.random.fold_in(key, 22), (block_count, 1, INNER_WIDTH), jnp.float32, -0.5, 0.5)
    offsets = jnp.broadcast_to(offsets, (block_count, TOK_DEV, INNER_WIDTH)).reshape(TOKENS, INNER_WIDTH)
    base_level = jnp.where(slow_cols, -11.0, -2.5)
    return (base_level[None, :] + jitter + offsets).astype(jnp.bfloat16)


def draw_correction_preact(key, part):
    slow_cols = head_pattern(key)
    fast_part = jax.random.uniform(jax.random.fold_in(key, 31), (TOKENS, INNER_WIDTH), jnp.float32, -3.0, 3.0)
    slow_part = jax.random.uniform(jax.random.fold_in(key, 32), (TOKENS, INNER_WIDTH), jnp.float32, -7.0, -5.0)
    return jnp.where(slow_cols[None, :], slow_part, fast_part).astype(jnp.bfloat16)


def block_levels(stream_key, shape, split, low, top_value):
    loudness = 1.0
    for axis_at, blocks in split:
        heights = jax.random.uniform(jax.random.fold_in(jax.random.fold_in(stream_key, 6), axis_at), (blocks,), jnp.float32, low / len(split), top_value / len(split))
        loudness = loudness * jnp.repeat(jnp.exp(heights), shape[axis_at] // blocks).reshape((-1,) + (1,) * (len(shape) - 1 - axis_at))
    return loudness


def assign_block(stream_key, own, number, rows, count, top, limit, skew):
    order = jax.random.permutation(stream_key, count)
    crowded, common = shares(count, rows * top, limit, skew, True), shares(count, rows * top, limit, skew, False)
    places = jnp.arange(count)

    def named(sizes, rotation):
        used = int((sizes > 0).sum())
        fixed = max(1, used // 4)
        passed = fixed + (places - fixed + rotation * (used - fixed)) % max(1, count - fixed)
        return jnp.zeros((count,), jnp.int32).at[order[jnp.where(places < fixed, places, passed)]].set(jnp.asarray(sizes, jnp.int32))

    sizes = jnp.where(number % 4 == 0, named(crowded, number // 4), named(common, number - number // 4 - 1))
    mixed = jax.random.permutation(jax.random.fold_in(own, 3), count)
    donor, taker = mixed[0:count // 2 * 2:2], mixed[1:count // 2 * 2:2]
    slack = jnp.minimum(sizes[donor] - 1, limit - sizes[taker]) // 2
    slack = jnp.where((donor == order[0]) | (taker == order[0]) | (sizes[taker] == 0), 0, jnp.maximum(slack, 0))
    passed = jax.random.randint(jax.random.fold_in(own, 4), (count // 2,), 0, 1 << 20) % (slack + 1)
    sizes = sizes.at[donor].add(-passed).at[taker].add(passed)
    members = jnp.searchsorted(jnp.cumsum(sizes), jnp.arange(rows * top), side="right").astype(jnp.int32)
    table = members.reshape(top, rows).T
    table = table[jax.random.permutation(jax.random.fold_in(own, 1), rows)]
    rotation = jax.random.randint(jax.random.fold_in(own, 2), (rows, 1), 0, top)
    return jnp.take_along_axis(table, (jnp.arange(top)[None, :] + rotation) % top, axis=1)


def shares(count, total, reach, skew, full):
    weights = [(1 << 20) // math.isqrt(rank ** skew) + 1 for rank in range(1, count + 1)]
    largest = reach if full else min(reach, max(-(-total // count), total * weights[0] // sum(weights)))
    least = 1 if total - largest >= count - 1 else 0
    given, spare = [largest] + [least] * (count - 1), total - largest - least * (count - 1)
    while spare > 0:
        movable = [i for i in range(1, count) if given[i] < largest] or [i for i in range(1, count) if given[i] < reach]
        mass, remaining = sum([weights[i] for i in movable]), spare
        for i in movable:
            more = min(reach - given[i], max(1, remaining * weights[i] // mass), spare)
            given[i] = given[i] + more
            spare = spare - more
    return np.array(given)


def noise(own_key, dims, width, bound, split=(), kind=jnp.bfloat16):
    values = jax.random.normal(own_key, dims, jnp.float32) * width
    if len(split) > 0:
        values = block_levels(own_key, dims, split, -0.22, 0.18) * values
    return jnp.clip(values, min=-bound, max=bound).astype(kind)


def setup_inputs(seed: int = 0) -> dict:
    keys = jax.random.split(jax.random.key(seed), 22)
    receptance = noise(keys[0], (TOKENS, INNER_WIDTH), 1.0, 6.0, ((0, 8), (1, 4)))
    key_by_head = noise(keys[1], (TOKENS, INNER_WIDTH), 1.0, 6.0, ((0, 8), (1, 4)))
    value_head_rows = noise(keys[2], (TOKENS, INNER_WIDTH), 1.0, 6.0, ((0, 8), (1, 4)))
    decay_preact = draw_decay_preact(jax.random.fold_in(keys[21], 71), 0)
    correction_preact = draw_correction_preact(jax.random.fold_in(keys[21], 71), 0)
    result_sigmoid_factor = noise(keys[5], (TOKENS, INNER_WIDTH), 1.0, 6.0, ((0, 8), (1, 4)))
    key_rate_mixing = jnp.clip(0.3 + 0.59999996 * jax.random.uniform(keys[6], (INNER_WIDTH,), jnp.float32) ** block_levels(keys[6], (INNER_WIDTH,), ((0, 4),), -0.2, 0.2), 0.3, 0.9)
    diagonal_current_factor = noise(keys[7], (INNER_WIDTH,), 0.12, 0.6, ((0, 4),), jnp.float32)
    per_head_gain = jnp.clip(1.0 + 0.18 * jax.random.normal(keys[8], (INNER_WIDTH,), jnp.float32), 0.1, 1.9)
    per_head_bias = noise(keys[9], (INNER_WIDTH,), 0.3, 1.5, ((0, 4),), jnp.float32)
    output_matrix = noise(keys[10], (INNER_WIDTH, D), INNER_WIDTH ** -0.5, 0.1875, ((0, 4),))
    residual = noise(keys[11], (TOKENS, D), 1.0, 6.0, ((0, 8),))
    expert_norm_gain = jnp.clip(1.0 + 0.18 * jax.random.normal(keys[12], (D,), jnp.float32), 0.1, 1.9)
    routes_keys = jax.random.split(jax.random.fold_in(keys[13], 1), TOKENS // TOK_DEV)
    routes_turns = jax.random.permutation(jax.random.fold_in(keys[13], 3), TOKENS // TOK_DEV)
    routes = jax.vmap(lambda own, number: assign_block(jax.random.fold_in(keys[13], 2), own, number, TOK_DEV, EXPERTS, TOP_K, CAP, 2))(routes_keys, routes_turns).reshape((TOKENS, TOP_K))
    chosen_expert_weight = jnp.clip(0.05 + 0.55 * jax.random.uniform(keys[14], (TOKENS, TOP_K), jnp.float32) ** block_levels(keys[14], (TOKENS, TOP_K), ((0, 8),), -0.2, 0.2), 0.05, 0.6)
    routed_gate_weight = noise(keys[15], (EXPERTS, D, FF), D ** -0.5, 0.125, ((0, 32),))
    routed_up_weight = noise(keys[16], (EXPERTS, D, FF), D ** -0.5, 0.125, ((0, 32),))
    routed_down_weight = noise(keys[17], (EXPERTS, FF, D), FF ** -0.5, 0.25, ((0, 32),))
    common_gate_weight = noise(keys[18], (D, FF), D ** -0.5, 0.125, ((1, 4),))
    common_up_weight = noise(keys[19], (D, FF), D ** -0.5, 0.125, ((1, 4),))
    common_down_weight = noise(keys[20], (FF, D), FF ** -0.5, 0.25, ((0, 4),))
    return {"receptance": receptance, "key_by_head": key_by_head, "value_head_rows": value_head_rows, "decay_preact": decay_preact, "correction_preact": correction_preact, "result_sigmoid_factor": result_sigmoid_factor, "key_rate_mixing": key_rate_mixing, "diagonal_current_factor": diagonal_current_factor, "per_head_gain": per_head_gain, "per_head_bias": per_head_bias, "output_matrix": output_matrix, "residual": residual, "expert_norm_gain": expert_norm_gain, "routes": routes, "chosen_expert_weight": chosen_expert_weight, "routed_gate_weight": routed_gate_weight, "routed_up_weight": routed_up_weight, "routed_down_weight": routed_down_weight, "common_gate_weight": common_gate_weight, "common_up_weight": common_up_weight, "common_down_weight": common_down_weight}


NORM_EPS = 1e-06
GROUP_EPS = 0.00064
HIGHEST = lax.Precision.HIGHEST

def partition_channels(source, head_size):
    row_count, col_count = source.shape
    return source.astype(jnp.float32).reshape(row_count, col_count // head_size, head_size)

def prepare(receptance, key_by_head, value_head_rows, decay_preact, correction_preact, key_rate_mixing):
    key_rows = partition_channels(key_by_head, CHANNEL_SPAN)
    learning = jax.nn.sigmoid(partition_channels(correction_preact, CHANNEL_SPAN))
    length = jnp.sqrt(lax.optimization_barrier(jnp.sum(key_rows * key_rows, axis=-1, keepdims=True)))
    unit_keys = key_rows / jnp.maximum(length, 1.0)
    mix_rows = key_rate_mixing.astype(jnp.float32).reshape(1, key_rows.shape[1], CHANNEL_SPAN)
    interpolated_lookup_vectors = key_rows * (1.0 + (learning - 1.0) * mix_rows)
    log_decay = -jnp.exp(-jax.nn.softplus(-partition_channels(decay_preact, CHANNEL_SPAN)) - 0.5)
    return (partition_channels(receptance, CHANNEL_SPAN), interpolated_lookup_vectors, partition_channels(value_head_rows, CHANNEL_SPAN), log_decay, unit_keys, learning)

def finalize(state_readout, query_vectors_partitioned, interpolated_lookup_vectors, content_vectors_partitioned, per_head_gain, per_head_bias, diagonal_current_factor, result_sigmoid_factor):
    shard_attention_count = state_readout.shape[1]
    average = lax.optimization_barrier(jnp.mean(state_readout, axis=-1, keepdims=True))
    centred = state_readout - average
    variance = lax.optimization_barrier(jnp.mean(centred * centred, axis=-1, keepdims=True))
    standardized_channels = centred * lax.rsqrt(variance + GROUP_EPS)
    standardized_channels = standardized_channels * per_head_gain.astype(jnp.float32).reshape(1, shard_attention_count, CHANNEL_SPAN) + per_head_bias.astype(jnp.float32).reshape(1, shard_attention_count, CHANNEL_SPAN)
    diagonal_extra_contribution = lax.optimization_barrier(jnp.sum(query_vectors_partitioned * interpolated_lookup_vectors * diagonal_current_factor.astype(jnp.float32).reshape(1, shard_attention_count, CHANNEL_SPAN), axis=-1, keepdims=True)) * content_vectors_partitioned
    concatenated_channels = (standardized_channels + diagonal_extra_contribution) * partition_channels(result_sigmoid_factor, CHANNEL_SPAN)
    return concatenated_channels.reshape(state_readout.shape[0], shard_attention_count * CHANNEL_SPAN).astype(jnp.bfloat16)

def expert_apply(rows_in, gate_weight, up_weight, down_weight):
    gate_part = jnp.dot(rows_in, gate_weight, preferred_element_type=jnp.float32)
    up_part = jnp.dot(rows_in, up_weight, preferred_element_type=jnp.float32)
    hidden = (jax.nn.silu(gate_part) * up_part).astype(jnp.bfloat16)
    return jnp.dot(hidden, down_weight, preferred_element_type=jnp.float32)

def reference(receptance, key_by_head, value_head_rows, decay_preact, correction_preact, result_sigmoid_factor, key_rate_mixing, diagonal_current_factor, per_head_gain, per_head_bias, output_matrix, residual, expert_norm_gain, routes, chosen_expert_weight, routed_gate_weight, routed_up_weight, routed_down_weight, common_gate_weight, common_up_weight, common_down_weight):
    query_vectors_partitioned, interpolated_lookup_vectors, content_vectors_partitioned, log_decay, unit_keys, learning = prepare(receptance, key_by_head, value_head_rows, decay_preact, correction_preact, key_rate_mixing)
    decay = jnp.exp(log_decay)

    def advance(memory, inputs):
        recept_now, key_now, value_now, decay_now, unit_now, learn_now = inputs
        erased = jnp.einsum('hij,hj->hi', memory, -unit_now, precision=HIGHEST)
        memory = memory * decay_now[:, None, :] + erased[:, :, None] * (unit_now * learn_now)[:, None, :] + value_now[:, :, None] * key_now[:, None, :]
        return (memory, jnp.einsum('hij,hj->hi', memory, recept_now, precision=HIGHEST))
    start_memory = jnp.zeros((HEADS, CHANNEL_SPAN, CHANNEL_SPAN), jnp.float32)
    final_memory, state_readout = lax.scan(advance, start_memory, (query_vectors_partitioned, interpolated_lookup_vectors, content_vectors_partitioned, decay, unit_keys, learning))
    blended_heads = finalize(state_readout, query_vectors_partitioned, interpolated_lookup_vectors, content_vectors_partitioned, per_head_gain, per_head_bias, diagonal_current_factor, result_sigmoid_factor)
    projected = jnp.dot(blended_heads, output_matrix, preferred_element_type=jnp.float32)
    middle = (residual.astype(jnp.float32) + projected).astype(jnp.bfloat16)
    middle_full = middle.astype(jnp.float32)
    row_scale = lax.rsqrt(lax.optimization_barrier(jnp.mean(middle_full * middle_full, axis=-1, keepdims=True)) + NORM_EPS)
    normed = (middle_full * row_scale * expert_norm_gain.astype(jnp.float32)).astype(jnp.bfloat16)
    shared_out = expert_apply(normed, common_gate_weight, common_up_weight, common_down_weight)
    slot_total = N_SP * CAP
    padded = jnp.concatenate([normed, jnp.zeros((1, D), normed.dtype)], axis=0)

    def one_expert(running, inputs):
        number, gate_weight, up_weight, down_weight = inputs
        matches = routes == number
        weight_row = lax.optimization_barrier(jnp.sum(jnp.where(matches, chosen_expert_weight, 0.0), axis=1))
        struck = jnp.any(matches, axis=1)
        index_rows = jnp.nonzero(struck, size=slot_total, fill_value=TOKENS)[0].astype(jnp.int32)
        answer = expert_apply(padded[index_rows], gate_weight, up_weight, down_weight).astype(jnp.bfloat16)
        weight_pad = jnp.concatenate([weight_row, jnp.zeros((1,), weight_row.dtype)], axis=0)
        running = running.at[index_rows].add(answer.astype(jnp.float32) * weight_pad[index_rows][:, None])
        return (running, None)
    routed_pad, unused = lax.scan(one_expert, jnp.zeros((TOKENS + 1, D), jnp.float32), (jnp.arange(EXPERTS, dtype=jnp.int32), routed_gate_weight, routed_up_weight, routed_down_weight))
    routed = routed_pad[:TOKENS]
    return (middle.astype(jnp.float32) + shared_out + routed).astype(jnp.bfloat16)
```

```python
import functools

import jax
import jax.numpy as jnp
from jax import lax
from jax.experimental import pallas as pl
from jax.experimental.pallas import tpu as pltpu
from jax.sharding import PartitionSpec as P

CHANNEL_SPAN = 64


NORM_EPS = 1e-06
GROUP_EPS = 0.00064
HIGHEST = lax.Precision.HIGHEST
STATE_TYPE = jnp.bfloat16

MESH = pl.DeviceIdType.MESH
VMEM_LIMIT = 60 * 1024 * 1024


def dot_nn(a, b):
    return lax.dot_general(
        a, b, (((1,), (0,)), ((), ())), precision=HIGHEST, preferred_element_type=jnp.float32
    )


def dot_nt(a, b):
    return lax.dot_general(
        a, b, (((1,), (1,)), ((), ())), precision=HIGHEST, preferred_element_type=jnp.float32
    )


def head_ones(width):
    row = lax.broadcasted_iota(jnp.int32, (width, width), 0) // CHANNEL_SPAN
    col = lax.broadcasted_iota(jnp.int32, (width, width), 1) // CHANNEL_SPAN
    return row == col


def memory_kernel(
    n_sp,
    n_tp,
    r_ref,
    k_ref,
    v_ref,
    d_ref,
    c_ref,
    g_ref,
    mix_ref,
    dcf_ref,
    gain_ref,
    bias_ref,
    w_ref,
    res_ref,
    ng_ref,
    mid_ref,
    nrm_ref,
    wbuf,
    outbox,
    inbox,
    heads,
    w_send,
    w_recv,
    f_send,
    f_recv,
    s_send,
    s_recv,
    h_send,
    h_recv,
    own_sem,
    kept,
    state,
):
    me, t = lax.axis_index("sp"), lax.axis_index("tp")
    tokens, width = r_ref.shape
    pair = 2 * CHANNEL_SPAN
    pairs = width // pair
    partner = t + 1 - 2 * lax.rem(t, 2)
    barrier = pltpu.get_barrier_semaphore()

    def greet_sp(i, carry):
        pl.semaphore_signal(
            barrier, inc=1, device_id={"sp": lax.rem(me + i, n_sp)}, device_id_type=MESH
        )
        return carry

    lax.fori_loop(1, n_sp, greet_sp, 0)
    for i in range(1, n_tp):
        pl.semaphore_signal(
            barrier, inc=1, device_id={"tp": lax.rem(t + i, n_tp)}, device_id_type=MESH
        )
    pl.semaphore_wait(barrier, n_sp - 1 + n_tp - 1)

    own = pltpu.make_async_copy(w_ref, wbuf.at[t], own_sem)
    own.start()
    w_copies = []
    for j in range(n_tp // 2):
        dest = partner if j == 0 else lax.rem(t + 2 * j, n_tp)
        copy = pltpu.make_async_remote_copy(
            src_ref=w_ref,
            dst_ref=wbuf.at[t],
            send_sem=w_send.at[j],
            recv_sem=w_recv.at[j],
            device_id={"tp": dest},
            device_id_type=MESH,
        )
        copy.start()
        w_copies.append(copy)

    f32 = jnp.float32
    row = lax.broadcasted_iota(jnp.int32, (tokens, tokens), 0)
    col = lax.broadcasted_iota(jnp.int32, (tokens, tokens), 1)
    strict = row > col
    inclusive = row >= col
    tri = jnp.where(inclusive, 1.0, 0.0).astype(f32)
    blk = head_ones(pair)
    ones_blk = jnp.where(blk, 1.0, 0.0).astype(f32)
    eye = jnp.where(
        lax.broadcasted_iota(jnp.int32, (pair, pair), 0)
        == lax.broadcasted_iota(jnp.int32, (pair, pair), 1),
        1.0,
        0.0,
    ).astype(f32)
    eye_tok = jnp.where(row == col, 1.0, 0.0).astype(f32)
    lane_head = lax.broadcasted_iota(jnp.int32, (1, pair), 1) // CHANNEL_SPAN
    lane_masks = [jnp.where(lane_head == h, 1.0, 0.0).astype(f32) for h in range(2)]

    for p in range(pairs):
        cols = pl.ds(p * pair, pair)
        recept = r_ref[:, cols].astype(f32)
        key = k_ref[:, cols].astype(f32)
        val = v_ref[:, cols].astype(f32)
        learning = 1.0 / (1.0 + jnp.exp(-c_ref[:, cols].astype(f32)))
        length = jnp.sqrt(dot_nn(key * key, ones_blk))
        unit = key / jnp.maximum(length, 1.0)
        mixed = key * (1.0 + (learning - 1.0) * mix_ref[:, cols])
        log_decay = -0.6065306597126334 / (1.0 + jnp.exp(-d_ref[:, cols].astype(f32)))
        cumulative = dot_nn(tri, log_decay)
        before = -jnp.exp(cumulative - log_decay) * unit
        inverse_decay = jnp.exp(-cumulative)
        erase = inverse_decay * unit * learning
        write = inverse_decay * mixed
        read = jnp.exp(cumulative) * recept
        removed = jnp.zeros((tokens, pair), f32)
        carried = jnp.zeros((tokens, pair), f32)
        pairs_re = []
        pairs_rw = []
        right = jnp.concatenate([erase, write], axis=0)
        for h in range(2):
            left = jnp.concatenate([before * lane_masks[h], read * lane_masks[h]], axis=0)
            prods = dot_nt(left, right)
            erase_pairs = jnp.where(strict, prods[:tokens, :tokens], 0.0)
            write_pairs = jnp.where(strict, prods[:tokens, tokens:], 0.0)
            pairs_re.append(jnp.where(inclusive, prods[tokens:, :tokens], 0.0))
            pairs_rw.append(jnp.where(inclusive, prods[tokens:, tokens:], 0.0))
            inverse = eye_tok + jnp.where(row // 2 == col // 2, erase_pairs, 0.0)
            block = 2
            while block < tokens:
                step = jnp.where(
                    (row // (2 * block) == col // (2 * block)) & (row // block != col // block),
                    erase_pairs,
                    0.0,
                )
                inverse = inverse + dot_nn(dot_nn(inverse, step), inverse)
                block *= 2
            rhs = jnp.concatenate([dot_nn(write_pairs, val), before], axis=1)
            solved = dot_nn(inverse, rhs)
            removed = removed + lane_masks[h] * solved[:, :pair]
            carried = carried + lane_masks[h] * solved[:, pair:]
        local_out = jnp.zeros((tokens, pair), f32)
        query = read
        both = jnp.concatenate([removed, carried], axis=1)
        for h in range(2):
            got = dot_nn(pairs_re[h], both)
            local_out = local_out + lane_masks[h] * (got[:, :pair] + dot_nn(pairs_rw[h], val))
            query = query + lane_masks[h] * got[:, pair:]
        final_decay = jnp.exp(cumulative[tokens - 1 : tokens, :])
        erase_end = final_decay * erase
        write_end = final_decay * write
        transit = jnp.where(blk, dot_nn(carried.T, erase_end), 0.0) + eye * final_decay
        contrib = jnp.where(
            blk, dot_nn(removed.T, erase_end) + dot_nn(val.T, write_end), 0.0
        )
        for at, full in ((0, transit), (1, contrib)):
            outbox[2 * p + at] = (full[:CHANNEL_SPAN] + full[CHANNEL_SPAN:]).astype(outbox.dtype)
        bonus = dot_nn(recept * mixed * dcf_ref[:, cols], ones_blk) * val
        kept[p, 0] = local_out
        kept[p, 1] = query
        kept[p, 2] = bonus
        state[p] = jnp.zeros((pair, pair), f32)

    def message(i):
        return pltpu.make_async_remote_copy(
            src_ref=outbox,
            dst_ref=inbox.at[me],
            send_sem=s_send.at[i],
            recv_sem=s_recv.at[me],
            device_id={"sp": i},
            device_id_type=MESH,
        )

    def send(i, carry):
        message(i).start()
        return carry

    lax.fori_loop(me + 1, n_sp, send, 0)

    def unpack(part):
        part = part.astype(f32)
        return jnp.concatenate([part * lane_masks[0], part * lane_masks[1]], axis=0)

    def hop(i, carry):
        pltpu.make_async_remote_copy(
            src_ref=outbox,
            dst_ref=inbox.at[i],
            send_sem=s_send.at[i],
            recv_sem=s_recv.at[i],
            device_id={"sp": i},
            device_id_type=MESH,
        ).wait_recv()
        for p in range(pairs):
            state[p] = dot_nn(state[p], unpack(inbox[i, 2 * p])) + unpack(inbox[i, 2 * p + 1])
        return carry

    lax.fori_loop(0, me, hop, 0)

    for p in range(pairs):
        cols = pl.ds(p * pair, pair)
        readout = kept[p, 0] + dot_nt(kept[p, 1], state[p])
        centred = readout - dot_nn(readout, ones_blk) * (1.0 / CHANNEL_SPAN)
        variance = dot_nn(centred * centred, ones_blk) * (1.0 / CHANNEL_SPAN)
        grouped = centred * lax.rsqrt(variance + GROUP_EPS) * gain_ref[:, cols] + bias_ref[:, cols]
        heads[t, :, cols] = ((grouped + kept[p, 2]) * g_ref[:, cols].astype(f32)).astype(jnp.bfloat16)

    h_copies = []
    for i in range(1, n_tp):
        copy = pltpu.make_async_remote_copy(
            src_ref=heads.at[t],
            dst_ref=heads.at[t],
            send_sem=h_send.at[i],
            recv_sem=h_recv.at[i],
            device_id={"tp": lax.rem(t + i, n_tp)},
            device_id_type=MESH,
        )
        copy.start()
        h_copies.append(copy)
    f_copies = []
    for j in range(1, n_tp // 2):
        w_copies[j].wait()
        source = lax.rem(t + n_tp - 2 * j, n_tp)
        copy = pltpu.make_async_remote_copy(
            src_ref=wbuf.at[source],
            dst_ref=wbuf.at[source],
            send_sem=f_send.at[j],
            recv_sem=f_recv.at[j],
            device_id={"tp": partner},
            device_id_type=MESH,
        )
        copy.start()
        f_copies.append(copy)
    own.wait()
    w_copies[0].wait()
    for copy in h_copies:
        copy.wait()
    for copy in f_copies:
        copy.wait()

    def drain(i, carry):
        message(i).wait_send()
        return carry

    lax.fori_loop(me + 1, n_sp, drain, 0)

    model = mid_ref.shape[1]
    whole = jnp.concatenate([heads[i] for i in range(n_tp)], axis=1)
    tile = min(512, model)
    square = jnp.zeros((tokens, 1), f32)
    for at in range(0, model, tile):
        wcol = jnp.concatenate([wbuf[i, :, at : at + tile] for i in range(n_tp)], axis=0)
        projected = jnp.dot(whole, wcol, preferred_element_type=f32)
        middle = (res_ref[:, at : at + tile].astype(f32) + projected).astype(jnp.bfloat16)
        mid_ref[:, at : at + tile] = middle
        wide = middle.astype(f32)
        square = square + jnp.sum(wide * wide, axis=1, keepdims=True)
    scale = lax.rsqrt(square * (1.0 / model) + NORM_EPS)
    for at in range(0, model, tile):
        wide = mid_ref[:, at : at + tile].astype(f32)
        nrm_ref[:, at : at + tile] = (wide * scale * ng_ref[:, at : at + tile]).astype(
            jnp.bfloat16
        )


def memory_and_norm(args):
    n_sp, n_tp = lax.axis_size("sp"), lax.axis_size("tp")
    r, k, v, d, c, g, mix, dcf, gain, bias, w, res, ng = args
    tokens, width = r.shape
    model = w.shape[1]
    pairs = width // (2 * CHANNEL_SPAN)
    dma = pltpu.SemaphoreType.DMA
    vm = pl.BlockSpec(memory_space=pltpu.VMEM)
    return pl.pallas_call(
        functools.partial(memory_kernel, n_sp, n_tp),
        out_shape=[jax.ShapeDtypeStruct((tokens, model), jnp.bfloat16)] * 2,
        in_specs=[vm] * 13,
        out_specs=[vm] * 2,
        scratch_shapes=[
            pltpu.VMEM((n_tp,) + w.shape, w.dtype),
            pltpu.VMEM((2 * pairs, CHANNEL_SPAN, 2 * CHANNEL_SPAN), STATE_TYPE),
            pltpu.VMEM((n_sp, 2 * pairs, CHANNEL_SPAN, 2 * CHANNEL_SPAN), STATE_TYPE),
            pltpu.VMEM((n_tp, tokens, width), jnp.bfloat16),
            dma((n_tp // 2,)),
            dma((n_tp // 2,)),
            dma((n_tp // 2,)),
            dma((n_tp // 2,)),
            dma((n_sp,)),
            dma((n_sp,)),
            dma((n_tp,)),
            dma((n_tp,)),
            dma,
            pltpu.VMEM((pairs, 3, tokens, 2 * CHANNEL_SPAN), jnp.float32),
            pltpu.VMEM((pairs, 2 * CHANNEL_SPAN, 2 * CHANNEL_SPAN), jnp.float32),
        ],
        compiler_params=pltpu.CompilerParams(
            collective_id=0, has_side_effects=True, vmem_limit_bytes=VMEM_LIMIT
        ),
        name="memory_and_norm",
    )(
        r, k, v, d, c, g,
        mix.reshape(1, -1), dcf.reshape(1, -1), gain.reshape(1, -1), bias.reshape(1, -1),
        w, res, ng.reshape(1, -1),
    )


def expert_apply(rows_in, gate_weight, up_weight, down_weight):
    gate_part = jnp.dot(rows_in, gate_weight, preferred_element_type=jnp.float32)
    up_part = jnp.dot(rows_in, up_weight, preferred_element_type=jnp.float32)
    hidden = (jax.nn.silu(gate_part) * up_part).astype(jnp.bfloat16)
    return jnp.dot(hidden, down_weight, preferred_element_type=jnp.float32)


def per_device(
    receptance,
    key_by_head,
    value_head_rows,
    decay_preact,
    correction_preact,
    result_sigmoid_factor,
    key_rate_mixing,
    diagonal_current_factor,
    per_head_gain,
    per_head_bias,
    output_matrix,
    residual,
    expert_norm_gain,
    routes,
    chosen_expert_weight,
    routed_gate_weight,
    routed_up_weight,
    routed_down_weight,
    common_gate_weight,
    common_up_weight,
    common_down_weight,
):
    middle, normed = memory_and_norm(
        (
            receptance,
            key_by_head,
            value_head_rows,
            decay_preact,
            correction_preact,
            result_sigmoid_factor,
            key_rate_mixing,
            diagonal_current_factor,
            per_head_gain,
            per_head_bias,
            output_matrix,
            residual,
            expert_norm_gain,
        )
    )
    tp_index = lax.axis_index("tp")
    tp_count = lax.axis_size("tp")
    sp_count = lax.axis_size("sp")
    token_count, top_count = routes.shape
    model_width = normed.shape[1]
    capacity = 3 * token_count * top_count // (2 * sp_count * tp_count)
    owned_routes = routes % tp_count == tp_index
    target = routes // tp_count
    places = jnp.arange(sp_count, dtype=jnp.int32)
    hit_counts = jnp.sum(
        jnp.where(owned_routes[:, :, None] & (target[:, :, None] == places[None, None, :]), 1, 0),
        axis=1,
    ).astype(jnp.int32)
    earlier = jnp.cumsum(hit_counts, axis=0) - hit_counts
    within = jnp.take_along_axis(earlier, target, axis=1)
    slot_index = target * capacity + within
    dropped = sp_count * capacity
    flat_slots = jnp.where(owned_routes, slot_index, dropped).reshape(-1)
    token_ids = jnp.broadcast_to(jnp.arange(token_count, dtype=jnp.int32)[:, None], routes.shape)
    slot_tokens = (
        jnp.full((dropped,), token_count, jnp.int32)
        .at[flat_slots]
        .set(token_ids.reshape(-1), mode="drop")
    )
    slot_weights = (
        jnp.zeros((dropped,), jnp.float32)
        .at[flat_slots]
        .set(chosen_expert_weight.reshape(-1), mode="drop")
    )
    padded = jnp.concatenate([normed, jnp.zeros((1, model_width), jnp.bfloat16)], axis=0)
    outgoing = padded[slot_tokens].reshape(sp_count, capacity, model_width)
    arrived = lax.all_to_all(outgoing, "sp", split_axis=0, concat_axis=0, tiled=True)
    source_count, item_count, feature_count = arrived.shape
    flat_rows = arrived.reshape(source_count * item_count, feature_count)
    answer = expert_apply(
        flat_rows, routed_gate_weight[0], routed_up_weight[0], routed_down_weight[0]
    ).astype(jnp.bfloat16)
    returned = lax.all_to_all(
        answer.reshape(source_count, item_count, feature_count),
        "sp",
        split_axis=0,
        concat_axis=0,
        tiled=True,
    )
    flat_back = returned.reshape(dropped, model_width)
    token_rows = jnp.arange(token_count, dtype=jnp.int32)
    combine_table = jnp.where(
        slot_tokens[None, :] == token_rows[:, None], slot_weights[None, :], 0.0
    )
    routed = jnp.dot(combine_table, flat_back.astype(jnp.float32), precision=HIGHEST)
    shared_out = expert_apply(normed, common_gate_weight, common_up_weight, common_down_weight)
    summed = lax.psum_scatter(
        (routed + shared_out).astype(jnp.bfloat16), "tp", scatter_dimension=1, tiled=True
    ).astype(jnp.float32)
    col_count = summed.shape[1]
    own_cols = lax.dynamic_slice_in_dim(middle, tp_index * col_count, col_count, 1)
    return (own_cols.astype(jnp.float32) + summed).astype(jnp.bfloat16)


def solution(mesh):
    return jax.shard_map(
        per_device,
        mesh=mesh,
        in_specs=(
            P("sp", "tp"),
            P("sp", "tp"),
            P("sp", "tp"),
            P("sp", "tp"),
            P("sp", "tp"),
            P("sp", "tp"),
            P("tp"),
            P("tp"),
            P("tp"),
            P("tp"),
            P("tp", None),
            P("sp", None),
            P(),
            P("sp", None),
            P("sp", None),
            P(("sp", "tp"), None, None),
            P(("sp", "tp"), None, None),
            P(("sp", "tp"), None, None),
            P(None, "tp"),
            P(None, "tp"),
            P("tp", None),
        ),
        out_specs=P("sp", "tp"),
        check_vma=False,
    )
```

```python
import functools

import jax
import jax.numpy as jnp
from jax import lax
from jax.experimental import pallas as pl
from jax.experimental.pallas import tpu as pltpu
from jax.sharding import PartitionSpec as P

CHANNEL_SPAN = 64


NORM_EPS = 1e-06
GROUP_EPS = 0.00064
HIGHEST = lax.Precision.HIGHEST
STATE_TYPE = jnp.bfloat16

MESH = pl.DeviceIdType.MESH
VMEM_LIMIT = 60 * 1024 * 1024


def dot_nn(a, b):
    return lax.dot_general(
        a, b, (((1,), (0,)), ((), ())), precision=HIGHEST, preferred_element_type=jnp.float32
    )


def dot_nt(a, b):
    return lax.dot_general(
        a, b, (((1,), (1,)), ((), ())), precision=HIGHEST, preferred_element_type=jnp.float32
    )


def head_ones(width):
    row = lax.broadcasted_iota(jnp.int32, (width, width), 0) // CHANNEL_SPAN
    col = lax.broadcasted_iota(jnp.int32, (width, width), 1) // CHANNEL_SPAN
    return row == col


def memory_kernel(
    n_sp,
    n_tp,
    r_ref,
    k_ref,
    v_ref,
    d_ref,
    c_ref,
    g_ref,
    mix_ref,
    dcf_ref,
    gain_ref,
    bias_ref,
    w_ref,
    res_ref,
    ng_ref,
    mid_ref,
    nrm_ref,
    wbuf,
    outbox,
    inbox,
    heads,
    w_send,
    w_recv,
    f_send,
    f_recv,
    s_send,
    s_recv,
    h_send,
    h_recv,
    own_sem,
    kept,
    state,
):
    me, t = lax.axis_index("sp"), lax.axis_index("tp")
    tokens, width = r_ref.shape
    pair = 2 * CHANNEL_SPAN
    pairs = width // pair
    partner = t + 1 - 2 * lax.rem(t, 2)
    barrier = pltpu.get_barrier_semaphore()

    def greet_sp(i, carry):
        pl.semaphore_signal(
            barrier, inc=1, device_id={"sp": lax.rem(me + i, n_sp)}, device_id_type=MESH
        )
        return carry

    lax.fori_loop(1, n_sp, greet_sp, 0)
    for i in range(1, n_tp):
        pl.semaphore_signal(
            barrier, inc=1, device_id={"tp": lax.rem(t + i, n_tp)}, device_id_type=MESH
        )
    pl.semaphore_wait(barrier, n_sp - 1 + n_tp - 1)

    own = pltpu.make_async_copy(w_ref, wbuf.at[t], own_sem)
    own.start()
    w_copies = []
    for j in range(n_tp // 2):
        dest = partner if j == 0 else lax.rem(t + 2 * j, n_tp)
        copy = pltpu.make_async_remote_copy(
            src_ref=w_ref,
            dst_ref=wbuf.at[t],
            send_sem=w_send.at[j],
            recv_sem=w_recv.at[j],
            device_id={"tp": dest},
            device_id_type=MESH,
        )
        copy.start()
        w_copies.append(copy)

    f32 = jnp.float32
    row = lax.broadcasted_iota(jnp.int32, (tokens, tokens), 0)
    col = lax.broadcasted_iota(jnp.int32, (tokens, tokens), 1)
    strict = row > col
    inclusive = row >= col
    tri = jnp.where(inclusive, 1.0, 0.0).astype(f32)
    blk = head_ones(pair)
    ones_blk = jnp.where(blk, 1.0, 0.0).astype(f32)
    eye = jnp.where(
        lax.broadcasted_iota(jnp.int32, (pair, pair), 0)
        == lax.broadcasted_iota(jnp.int32, (pair, pair), 1),
        1.0,
        0.0,
    ).astype(f32)
    eye_tok = jnp.where(row == col, 1.0, 0.0).astype(f32)
    lane_head = lax.broadcasted_iota(jnp.int32, (1, pair), 1) // CHANNEL_SPAN
    lane_masks = [jnp.where(lane_head == h, 1.0, 0.0).astype(f32) for h in range(2)]

    for p in range(pairs):
        cols = pl.ds(p * pair, pair)
        recept = r_ref[:, cols].astype(f32)
        key = k_ref[:, cols].astype(f32)
        val = v_ref[:, cols].astype(f32)
        learning = 1.0 / (1.0 + jnp.exp(-c_ref[:, cols].astype(f32)))
        length = jnp.sqrt(dot_nn(key * key, ones_blk))
        unit = key / jnp.maximum(length, 1.0)
        mixed = key * (1.0 + (learning - 1.0) * mix_ref[:, cols])
        log_decay = -0.6065306597126334 / (1.0 + jnp.exp(-d_ref[:, cols].astype(f32)))
        cumulative = dot_nn(tri, log_decay)
        before = -jnp.exp(cumulative - log_decay) * unit
        inverse_decay = jnp.exp(-cumulative)
        erase = inverse_decay * unit * learning
        write = inverse_decay * mixed
        read = jnp.exp(cumulative) * recept
        removed = jnp.zeros((tokens, pair), f32)
        carried = jnp.zeros((tokens, pair), f32)
        pairs_re = []
        pairs_rw = []
        right = jnp.concatenate([erase, write], axis=0)
        for h in range(2):
            left = jnp.concatenate([before * lane_masks[h], read * lane_masks[h]], axis=0)
            prods = dot_nt(left, right)
            erase_pairs = jnp.where(strict, prods[:tokens, :tokens], 0.0)
            write_pairs = jnp.where(strict, prods[:tokens, tokens:], 0.0)
            pairs_re.append(jnp.where(inclusive, prods[tokens:, :tokens], 0.0))
            pairs_rw.append(jnp.where(inclusive, prods[tokens:, tokens:], 0.0))
            inverse = eye_tok + jnp.where(row // 2 == col // 2, erase_pairs, 0.0)
            block = 2
            while block < tokens:
                step = jnp.where(
                    (row // (2 * block) == col // (2 * block)) & (row // block != col // block),
                    erase_pairs,
                    0.0,
                )
                inverse = inverse + dot_nn(dot_nn(inverse, step), inverse)
                block *= 2
            rhs = jnp.concatenate([dot_nn(write_pairs, val), before], axis=1)
            solved = dot_nn(inverse, rhs)
            removed = removed + lane_masks[h] * solved[:, :pair]
            carried = carried + lane_masks[h] * solved[:, pair:]
        local_out = jnp.zeros((tokens, pair), f32)
        query = read
        both = jnp.concatenate([removed, carried], axis=1)
        for h in range(2):
            got = dot_nn(pairs_re[h], both)
            local_out = local_out + lane_masks[h] * (got[:, :pair] + dot_nn(pairs_rw[h], val))
            query = query + lane_masks[h] * got[:, pair:]
        final_decay = jnp.exp(cumulative[tokens - 1 : tokens, :])
        erase_end = final_decay * erase
        write_end = final_decay * write
        transit = jnp.where(blk, dot_nn(carried.T, erase_end), 0.0) + eye * final_decay
        contrib = jnp.where(
            blk, dot_nn(removed.T, erase_end) + dot_nn(val.T, write_end), 0.0
        )
        for at, full in ((0, transit), (1, contrib)):
            outbox[2 * p + at] = (full[:CHANNEL_SPAN] + full[CHANNEL_SPAN:]).astype(outbox.dtype)
        bonus = dot_nn(recept * mixed * dcf_ref[:, cols], ones_blk) * val
        kept[p, 0] = local_out
        kept[p, 1] = query
        kept[p, 2] = bonus
        state[p] = jnp.zeros((pair, pair), f32)

    def message(i):
        return pltpu.make_async_remote_copy(
            src_ref=outbox,
            dst_ref=inbox.at[me],
            send_sem=s_send.at[i],
            recv_sem=s_recv.at[me],
            device_id={"sp": i},
            device_id_type=MESH,
        )

    def send(i, carry):
        message(i).start()
        return carry

    lax.fori_loop(me + 1, n_sp, send, 0)

    def unpack(part):
        part = part.astype(f32)
        return jnp.concatenate([part * lane_masks[0], part * lane_masks[1]], axis=0)

    def hop(i, carry):
        pltpu.make_async_remote_copy(
            src_ref=outbox,
            dst_ref=inbox.at[i],
            send_sem=s_send.at[i],
            recv_sem=s_recv.at[i],
            device_id={"sp": i},
            device_id_type=MESH,
        ).wait_recv()
        for p in range(pairs):
            state[p] = dot_nn(state[p], unpack(inbox[i, 2 * p])) + unpack(inbox[i, 2 * p + 1])
        return carry

    lax.fori_loop(0, me, hop, 0)

    for p in range(pairs):
        cols = pl.ds(p * pair, pair)
        readout = kept[p, 0] + dot_nt(kept[p, 1], state[p])
        centred = readout - dot_nn(readout, ones_blk) * (1.0 / CHANNEL_SPAN)
        variance = dot_nn(centred * centred, ones_blk) * (1.0 / CHANNEL_SPAN)
        grouped = centred * lax.rsqrt(variance + GROUP_EPS) * gain_ref[:, cols] + bias_ref[:, cols]
        heads[t, :, cols] = ((grouped + kept[p, 2]) * g_ref[:, cols].astype(f32)).astype(jnp.bfloat16)

    h_copies = []
    for i in range(1, n_tp):
        copy = pltpu.make_async_remote_copy(
            src_ref=heads.at[t],
            dst_ref=heads.at[t],
            send_sem=h_send.at[i],
            recv_sem=h_recv.at[i],
            device_id={"tp": lax.rem(t + i, n_tp)},
            device_id_type=MESH,
        )
        copy.start()
        h_copies.append(copy)
    f_copies = []
    for j in range(1, n_tp // 2):
        w_copies[j].wait()
        source = lax.rem(t + n_tp - 2 * j, n_tp)
        copy = pltpu.make_async_remote_copy(
            src_ref=wbuf.at[source],
            dst_ref=wbuf.at[source],
            send_sem=f_send.at[j],
            recv_sem=f_recv.at[j],
            device_id={"tp": partner},
            device_id_type=MESH,
        )
        copy.start()
        f_copies.append(copy)
    own.wait()
    w_copies[0].wait()
    for copy in h_copies:
        copy.wait()
    for copy in f_copies:
        copy.wait()

    def drain(i, carry):
        message(i).wait_send()
        return carry

    lax.fori_loop(me + 1, n_sp, drain, 0)

    model = mid_ref.shape[1]
    whole = jnp.concatenate([heads[i] for i in range(n_tp)], axis=1)
    tile = min(512, model)
    square = jnp.zeros((tokens, 1), f32)
    for at in range(0, model, tile):
        wcol = jnp.concatenate([wbuf[i, :, at : at + tile] for i in range(n_tp)], axis=0)
        projected = jnp.dot(whole, wcol, preferred_element_type=f32)
        middle = (res_ref[:, at : at + tile].astype(f32) + projected).astype(jnp.bfloat16)
        mid_ref[:, at : at + tile] = middle
        wide = middle.astype(f32)
        square = square + jnp.sum(wide * wide, axis=1, keepdims=True)
    scale = lax.rsqrt(square * (1.0 / model) + NORM_EPS)
    for at in range(0, model, tile):
        wide = mid_ref[:, at : at + tile].astype(f32)
        nrm_ref[:, at : at + tile] = (wide * scale * ng_ref[:, at : at + tile]).astype(
            jnp.bfloat16
        )


def memory_and_norm(args):
    n_sp, n_tp = lax.axis_size("sp"), lax.axis_size("tp")
    r, k, v, d, c, g, mix, dcf, gain, bias, w, res, ng = args
    tokens, width = r.shape
    model = w.shape[1]
    pairs = width // (2 * CHANNEL_SPAN)
    dma = pltpu.SemaphoreType.DMA
    vm = pl.BlockSpec(memory_space=pltpu.VMEM)
    return pl.pallas_call(
        functools.partial(memory_kernel, n_sp, n_tp),
        out_shape=[jax.ShapeDtypeStruct((tokens, model), jnp.bfloat16)] * 2,
        in_specs=[vm] * 13,
        out_specs=[vm] * 2,
        scratch_shapes=[
            pltpu.VMEM((n_tp,) + w.shape, w.dtype),
            pltpu.VMEM((2 * pairs, CHANNEL_SPAN, 2 * CHANNEL_SPAN), STATE_TYPE),
            pltpu.VMEM((n_sp, 2 * pairs, CHANNEL_SPAN, 2 * CHANNEL_SPAN), STATE_TYPE),
            pltpu.VMEM((n_tp, tokens, width), jnp.bfloat16),
            dma((n_tp // 2,)),
            dma((n_tp // 2,)),
            dma((n_tp // 2,)),
            dma((n_tp // 2,)),
            dma((n_sp,)),
            dma((n_sp,)),
            dma((n_tp,)),
            dma((n_tp,)),
            dma,
            pltpu.VMEM((pairs, 3, tokens, 2 * CHANNEL_SPAN), jnp.float32),
            pltpu.VMEM((pairs, 2 * CHANNEL_SPAN, 2 * CHANNEL_SPAN), jnp.float32),
        ],
        compiler_params=pltpu.CompilerParams(
            collective_id=0, has_side_effects=True, vmem_limit_bytes=VMEM_LIMIT
        ),
        name="memory_and_norm",
    )(
        r, k, v, d, c, g,
        mix.reshape(1, -1), dcf.reshape(1, -1), gain.reshape(1, -1), bias.reshape(1, -1),
        w, res, ng.reshape(1, -1),
    )


def expert_apply(rows_in, gate_weight, up_weight, down_weight):
    gate_part = jnp.dot(rows_in, gate_weight, preferred_element_type=jnp.float32)
    up_part = jnp.dot(rows_in, up_weight, preferred_element_type=jnp.float32)
    hidden = (jax.nn.silu(gate_part) * up_part).astype(jnp.bfloat16)
    return jnp.dot(hidden, down_weight, preferred_element_type=jnp.float32)


def expert_kernel(
    n_sp,
    n_tp,
    cap,
    nrm_ref,
    own_ref,
    wt_ref,
    gate_hbm,
    up_hbm,
    down_hbm,
    cg_ref,
    cu_ref,
    cd_ref,
    out_ref,
    gate,
    up,
    down,
    blocks,
    tables,
    shared,
    rows_in,
    part,
    core_in,
    y_out,
    y_in,
    kept,
    x_out,
    x_in,
    z_out,
    z_in,
    w_sem,
    t_send,
    t_recv,
    az_send,
    az_recv,
    ax_send,
    ax_recv,
    ay_send,
    ay_recv,
    ac_send,
    ac_recv,
    rc_send,
    rc_recv,
    ry_send,
    ry_recv,
    rx_send,
    rx_recv,
    rz_send,
    rz_recv,
):
    f32, bf16 = jnp.float32, jnp.bfloat16
    me, t = lax.axis_index("sp"), lax.axis_index("tp")
    tokens, model = nrm_ref.shape
    groups = n_sp // 2
    fars = n_tp // 2
    strip = tokens // n_tp
    cols = model // n_tp
    core_to = t + 1 - 2 * lax.rem(t, 2)
    x_to = me + 1 - 2 * lax.rem(me, 2)
    parity = lax.rem(t, 2)

    def remote(src, dst, send, recv, device):
        return pltpu.make_async_remote_copy(
            src_ref=src,
            dst_ref=dst,
            send_sem=send,
            recv_sem=recv,
            device_id=device,
            device_id_type=MESH,
        )

    barrier = pltpu.get_barrier_semaphore()

    def greet(i, carry):
        pl.semaphore_signal(
            barrier, inc=1, device_id={"sp": lax.rem(me + i, n_sp)}, device_id_type=MESH
        )
        return carry

    lax.fori_loop(1, n_sp, greet, 0)
    for i in range(1, n_tp):
        pl.semaphore_signal(
            barrier, inc=1, device_id={"tp": lax.rem(t + i, n_tp)}, device_id_type=MESH
        )
    loads = [
        pltpu.make_async_copy(src, dst, w_sem.at[i])
        for i, (src, dst) in enumerate(((gate_hbm, gate), (up_hbm, up), (down_hbm, down)))
    ]
    for load in loads:
        load.start()
    pl.semaphore_wait(barrier, n_sp - 1 + n_tp - 1)

    def source(j):
        return lax.rem(me + n_sp - 2 * j, n_sp)

    def near(b):
        return b + 1 - 2 * lax.rem(b, 2)

    def rows(b, q):
        return blocks.at[b, pl.ds(pl.multiple_of(q * strip, strip), strip)]

    def own_rows():
        return nrm_ref.at[pl.ds(pl.multiple_of(t * strip, strip), strip)]

    def table_copy(i):
        to = lax.rem(me + i, n_sp)
        return remote(wt_ref.at[to], tables.at[me], t_send.at[i], t_recv.at[i], {"sp": to})

    def z_copy(j):
        to = lax.rem(me + 2 * j, n_sp)
        return remote(own_rows(), rows(me, t), az_send.at[j], az_recv.at[j], {"sp": to})

    for i in range(1, n_sp):
        table_copy(i).start()
    blocks[me] = nrm_ref[...]
    tables[me] = wt_ref[me]

    def x_own():
        return remote(own_rows(), rows(me, t), ax_send.at[0], ax_recv.at[0], {"sp": x_to})

    def x_copy(j):
        b = source(j)
        return remote(rows(b, t), rows(b, t), ax_send.at[j], ax_recv.at[j], {"sp": x_to})

    def tp_copies(j, side):
        b = source(j) if side == 0 else near(source(j))
        return [
            remote(
                rows(b, t),
                rows(b, t),
                ay_send.at[j, side, k],
                ay_recv.at[j, side, k],
                {"tp": lax.rem(t + 2 * k, n_tp)},
            )
            for k in range(1, fars)
        ]

    def core_copies(j, side):
        b = source(j) if side == 0 else near(source(j))
        found = []
        for k in range(fars):
            q = lax.rem(t + n_tp - 2 * k, n_tp)
            found.append(
                remote(
                    rows(b, q),
                    rows(b, q),
                    ac_send.at[j, side, k],
                    ac_recv.at[j, side, k],
                    {"tp": core_to},
                )
            )
        return found

    x_own().start()
    for j in range(1, groups):
        z_copy(j).start()

    hid = jnp.dot(nrm_ref[...], cg_ref[...], preferred_element_type=f32)
    hid = hid / (1.0 + jnp.exp(-hid)) * jnp.dot(
        nrm_ref[...], cu_ref[...], preferred_element_type=f32
    )
    hid = hid.astype(bf16)
    for q in range(n_tp):
        shared[q] = jnp.dot(
            hid, cd_ref[:, q * cols : (q + 1) * cols], preferred_element_type=f32
        )
    for load in loads:
        load.wait()

    slot_row = lax.broadcasted_iota(jnp.int32, (cap, tokens), 0).astype(f32)
    earlier = jnp.where(
        lax.broadcasted_iota(jnp.int32, (tokens, tokens), 0)
        < lax.broadcasted_iota(jnp.int32, (tokens, tokens), 1),
        1.0,
        0.0,
    ).astype(bf16)

    def rc_copy(j, m):
        q = 2 * m + (1 - parity)
        return remote(
            part.at[j, q], core_in.at[j, m], rc_send.at[j, m], rc_recv.at[j, m], {"tp": core_to}
        )

    def ry_copy(j, k):
        return remote(
            y_out.at[j, k],
            y_in.at[j, k],
            ry_send.at[j, k],
            ry_recv.at[j, k],
            {"tp": lax.rem(t + 2 * k, n_tp)},
        )

    def rx_copy(j):
        return remote(x_out.at[j], x_in.at[j], rx_send.at[j], rx_recv.at[j], {"sp": x_to})

    def rz_copy(j):
        return remote(
            z_out.at[j], z_in.at[j], rz_send.at[j], rz_recv.at[j], {"sp": source(j)}
        )

    def z_stage(j):
        @pl.when(j > 0)
        def _():
            z_copy(j).wait_recv()
            x_copy(j).start()
            for copy in tp_copies(j, 0):
                copy.start()

    def x_stage(j):
        x_copy(j).wait_recv()
        for copy in tp_copies(j, 1):
            copy.start()

    def y_stage(j):
        @pl.when(j > 0)
        def _():
            for copy in tp_copies(j, 0):
                copy.wait_recv()
            for copy in core_copies(j, 0):
                copy.start()

        for copy in tp_copies(j, 1):
            copy.wait_recv()
        for copy in core_copies(j, 1):
            copy.start()

    def compute(j):
        @pl.when(j > 0)
        def _():
            for copy in core_copies(j, 0):
                copy.wait_recv()
            table_copy(2 * j).wait_recv()

        for copy in core_copies(j, 1):
            copy.wait_recv()
        b0 = source(j)
        b1 = near(b0)
        table_copy(lax.rem(me + n_sp - b1, n_sp)).wait_recv()
        weighted = []
        for side, b in ((0, b0), (1, b1)):
            w = tables[b]
            routed = jnp.where(w > 0.0, 1.0, 0.0).astype(bf16)
            rank = jnp.dot(routed, earlier, preferred_element_type=f32)
            hit = (slot_row == rank[0:1, :]) & (w[0:1, :] > 0.0)
            pick = jnp.where(hit, 1.0, 0.0).astype(bf16)
            full = jnp.where(hit, w[0:1, :], 0.0).T
            high = full.astype(bf16)
            low = (full - high.astype(f32)).astype(bf16)
            weighted.append((high, low))
            for q in range(n_tp):
                at = slice(q * cols, (q + 1) * cols)
                rows_in[side * cap : (side + 1) * cap, at] = jnp.dot(
                    pick, blocks[b, :, at], preferred_element_type=f32
                ).astype(bf16)
        x = rows_in[...]
        g = jnp.dot(x, gate[0], preferred_element_type=f32)
        u = jnp.dot(x, up[0], preferred_element_type=f32)
        hidden = (g / (1.0 + jnp.exp(-g)) * u).astype(bf16)
        first = jnp.where(j == 0, 1.0, 0.0).astype(f32)
        for q in range(n_tp):
            answer = jnp.dot(
                hidden, down[0, :, q * cols : (q + 1) * cols], preferred_element_type=f32
            ).astype(bf16)
            for side in range(2):
                high, low = weighted[side]
                a = answer[side * cap : (side + 1) * cap]
                total = jnp.dot(high, a, preferred_element_type=f32) + jnp.dot(
                    low, a, preferred_element_type=f32
                )
                if side == 0:
                    total = total + first * shared[q]
                part[j, q, side * tokens : (side + 1) * tokens] = total.astype(bf16)
        for m in range(fars):
            rc_copy(j, m).start()

    def core_stage(j):
        for m in range(fars):
            rc_copy(j, m).wait_recv()
        for k in range(1, fars):
            q = lax.rem(t + 2 * k, n_tp)
            y_out[j, k] = (
                part[j, q].astype(f32) + core_in[j, lax.div(q, 2)].astype(f32)
            ).astype(bf16)
            ry_copy(j, k).start()

    def y_reduce(j):
        for k in range(1, fars):
            ry_copy(j, k).wait_recv()
        for side in (1, 0):
            at = slice(side * tokens, (side + 1) * tokens)
            total = part[j, t, at].astype(f32) + core_in[j, lax.div(t, 2), at].astype(f32)
            for k in range(1, fars):
                total = total + y_in[j, k, at].astype(f32)
            if side == 1:
                x_out[j] = total.astype(bf16)
                rx_copy(j).start()
            else:
                kept[j] = total

    def x_reduce(j):
        rx_copy(j).wait_recv()
        kept[j] = kept[j] + x_in[j].astype(f32)

        @pl.when(j > 0)
        def _():
            z_out[j] = kept[j].astype(bf16)
            rz_copy(j).start()

    stages = (x_reduce, y_reduce, core_stage, compute, y_stage, x_stage, z_stage)
    lags = (6, 5, 4, 3, 2, 1, 0)

    def step(s, carry):
        for lag, stage in sorted(zip(lags, stages), key=lambda pair: pair[0]):

            @pl.when((s >= lag) & (s < groups + lag))
            def _():
                stage(s - lag)

        return carry

    lax.fori_loop(0, groups + lags[0], step, 0)

    total = kept[0] + own_ref[...].astype(f32)
    for j in range(1, groups):
        rz_copy(j).wait_recv()
        total = total + z_in[j].astype(f32)
    out_ref[...] = total.astype(out_ref.dtype)

    for i in range(1, n_sp):
        table_copy(i).wait_send()
    x_own().wait_send()
    for j in range(groups):
        if j > 0:
            z_copy(j).wait_send()
            x_copy(j).wait_send()
            rz_copy(j).wait_send()
        for side in range(2):
            if j > 0 or side > 0:
                for copy in tp_copies(j, side) + core_copies(j, side):
                    copy.wait_send()
        for m in range(fars):
            rc_copy(j, m).wait_send()
        for k in range(1, fars):
            ry_copy(j, k).wait_send()
        rx_copy(j).wait_send()


def expert_layer(normed, own_cols, weights, gate, up, down, cgate, cup, cdown, cap):
    n_sp, n_tp = lax.axis_size("sp"), lax.axis_size("tp")
    tokens, model = normed.shape
    groups, fars, cols = n_sp // 2, n_tp // 2, model // n_tp
    bf16, f32 = jnp.bfloat16, jnp.float32
    dma = pltpu.SemaphoreType.DMA
    vm = pl.BlockSpec(memory_space=pltpu.VMEM)
    hbm = pl.BlockSpec(memory_space=pl.ANY)
    pairs = [dma((n_sp,)), dma((n_sp,)), dma((groups,)), dma((groups,)), dma((groups,)), dma((groups,))]
    pairs += [dma((groups, 2, fars))] * 4
    pairs += [dma((groups, fars))] * 4
    pairs += [dma((groups,))] * 4
    return pl.pallas_call(
        functools.partial(expert_kernel, n_sp, n_tp, cap),
        out_shape=jax.ShapeDtypeStruct((tokens, cols), bf16),
        in_specs=[vm, vm, vm, hbm, hbm, hbm, vm, vm, vm],
        out_specs=vm,
        scratch_shapes=[
            pltpu.VMEM(gate.shape, bf16),
            pltpu.VMEM(up.shape, bf16),
            pltpu.VMEM(down.shape, bf16),
            pltpu.VMEM((n_sp, tokens, model), bf16),
            pltpu.VMEM(weights.shape, f32),
            pltpu.VMEM((n_tp, tokens, cols), f32),
            pltpu.VMEM((2 * cap, model), bf16),
            pltpu.VMEM((groups, n_tp, 2 * tokens, cols), bf16),
            pltpu.VMEM((groups, fars, 2 * tokens, cols), bf16),
            pltpu.VMEM((groups, fars, 2 * tokens, cols), bf16),
            pltpu.VMEM((groups, fars, 2 * tokens, cols), bf16),
            pltpu.VMEM((groups, tokens, cols), f32),
            pltpu.VMEM((groups, tokens, cols), bf16),
            pltpu.VMEM((groups, tokens, cols), bf16),
            pltpu.VMEM((groups, tokens, cols), bf16),
            pltpu.VMEM((groups, tokens, cols), bf16),
            dma((3,)),
        ]
        + pairs,
        compiler_params=pltpu.CompilerParams(
            collective_id=1, has_side_effects=True, vmem_limit_bytes=VMEM_LIMIT
        ),
        name="expert_layer",
    )(normed, own_cols, weights, gate, up, down, cgate, cup, cdown)


def per_device(
    receptance,
    key_by_head,
    value_head_rows,
    decay_preact,
    correction_preact,
    result_sigmoid_factor,
    key_rate_mixing,
    diagonal_current_factor,
    per_head_gain,
    per_head_bias,
    output_matrix,
    residual,
    expert_norm_gain,
    routes,
    chosen_expert_weight,
    routed_gate_weight,
    routed_up_weight,
    routed_down_weight,
    common_gate_weight,
    common_up_weight,
    common_down_weight,
):
    middle, normed = memory_and_norm(
        (
            receptance,
            key_by_head,
            value_head_rows,
            decay_preact,
            correction_preact,
            result_sigmoid_factor,
            key_rate_mixing,
            diagonal_current_factor,
            per_head_gain,
            per_head_bias,
            output_matrix,
            residual,
            expert_norm_gain,
        )
    )
    tp_index = lax.axis_index("tp")
    tp_count = lax.axis_size("tp")
    sp_count = lax.axis_size("sp")
    token_count, top_count = routes.shape
    model_width = normed.shape[1]
    capacity = 3 * token_count * top_count // (2 * sp_count * tp_count)
    held = sp_count * token_count * model_width * normed.dtype.itemsize
    if sp_count % 2 == 0 and tp_count % 2 == 0 and 6 * held <= VMEM_LIMIT:
        mine = jnp.arange(sp_count, dtype=jnp.int32) * tp_count + tp_index
        named = routes.T[None, :, :] == mine[:, None, None]
        weights = jnp.sum(jnp.where(named, chosen_expert_weight.T[None, :, :], 0.0), axis=1)
        weights = jnp.broadcast_to(weights[:, None, :], (sp_count, 8, token_count))
        col_count = model_width // tp_count
        own_cols = lax.dynamic_slice_in_dim(middle, tp_index * col_count, col_count, 1)
        return expert_layer(
            normed,
            own_cols,
            weights,
            routed_gate_weight,
            routed_up_weight,
            routed_down_weight,
            common_gate_weight,
            common_up_weight,
            common_down_weight,
            capacity,
        )
    owned_routes = routes % tp_count == tp_index
    target = routes // tp_count
    places = jnp.arange(sp_count, dtype=jnp.int32)
    hit_counts = jnp.sum(
        jnp.where(owned_routes[:, :, None] & (target[:, :, None] == places[None, None, :]), 1, 0),
        axis=1,
    ).astype(jnp.int32)
    earlier = jnp.cumsum(hit_counts, axis=0) - hit_counts
    within = jnp.take_along_axis(earlier, target, axis=1)
    slot_index = target * capacity + within
    dropped = sp_count * capacity
    flat_slots = jnp.where(owned_routes, slot_index, dropped).reshape(-1)
    token_ids = jnp.broadcast_to(jnp.arange(token_count, dtype=jnp.int32)[:, None], routes.shape)
    slot_tokens = (
        jnp.full((dropped,), token_count, jnp.int32)
        .at[flat_slots]
        .set(token_ids.reshape(-1), mode="drop")
    )
    slot_weights = (
        jnp.zeros((dropped,), jnp.float32)
        .at[flat_slots]
        .set(chosen_expert_weight.reshape(-1), mode="drop")
    )
    padded = jnp.concatenate([normed, jnp.zeros((1, model_width), jnp.bfloat16)], axis=0)
    outgoing = padded[slot_tokens].reshape(sp_count, capacity, model_width)
    arrived = lax.all_to_all(outgoing, "sp", split_axis=0, concat_axis=0, tiled=True)
    source_count, item_count, feature_count = arrived.shape
    flat_rows = arrived.reshape(source_count * item_count, feature_count)
    answer = expert_apply(
        flat_rows, routed_gate_weight[0], routed_up_weight[0], routed_down_weight[0]
    ).astype(jnp.bfloat16)
    returned = lax.all_to_all(
        answer.reshape(source_count, item_count, feature_count),
        "sp",
        split_axis=0,
        concat_axis=0,
        tiled=True,
    )
    flat_back = returned.reshape(dropped, model_width)
    token_rows = jnp.arange(token_count, dtype=jnp.int32)
    combine_table = jnp.where(
        slot_tokens[None, :] == token_rows[:, None], slot_weights[None, :], 0.0
    )
    routed = jnp.dot(combine_table, flat_back.astype(jnp.float32), precision=HIGHEST)
    shared_out = expert_apply(normed, common_gate_weight, common_up_weight, common_down_weight)
    summed = lax.psum_scatter(
        (routed + shared_out).astype(jnp.bfloat16), "tp", scatter_dimension=1, tiled=True
    ).astype(jnp.float32)
    col_count = summed.shape[1]
    own_cols = lax.dynamic_slice_in_dim(middle, tp_index * col_count, col_count, 1)
    return (own_cols.astype(jnp.float32) + summed).astype(jnp.bfloat16)


def solution(mesh):
    return jax.shard_map(
        per_device,
        mesh=mesh,
        in_specs=(
            P("sp", "tp"),
            P("sp", "tp"),
            P("sp", "tp"),
            P("sp", "tp"),
            P("sp", "tp"),
            P("sp", "tp"),
            P("tp"),
            P("tp"),
            P("tp"),
            P("tp"),
            P("tp", None),
            P("sp", None),
            P(),
            P("sp", None),
            P("sp", None),
            P(("sp", "tp"), None, None),
            P(("sp", "tp"), None, None),
            P(("sp", "tp"), None, None),
            P(None, "tp"),
            P(None, "tp"),
            P("tp", None),
        ),
        out_specs=P("sp", "tp"),
        check_vma=False,
    )
```

```python
import functools

import jax
import jax.numpy as jnp
from jax import lax
from jax.experimental import pallas as pl
from jax.experimental.pallas import tpu as pltpu
from jax.sharding import PartitionSpec as P

CHANNEL_SPAN = 64


NORM_EPS = 1e-06
GROUP_EPS = 0.00064
HIGHEST = lax.Precision.HIGHEST
STATE_TYPE = jnp.bfloat16

MESH = pl.DeviceIdType.MESH
VMEM_LIMIT = 60 * 1024 * 1024


def dot_nn(a, b):
    return lax.dot_general(
        a, b, (((1,), (0,)), ((), ())), precision=HIGHEST, preferred_element_type=jnp.float32
    )


def dot_nt(a, b):
    return lax.dot_general(
        a, b, (((1,), (1,)), ((), ())), precision=HIGHEST, preferred_element_type=jnp.float32
    )


def head_ones(width):
    row = lax.broadcasted_iota(jnp.int32, (width, width), 0) // CHANNEL_SPAN
    col = lax.broadcasted_iota(jnp.int32, (width, width), 1) // CHANNEL_SPAN
    return row == col


def memory_kernel(
    n_sp,
    n_tp,
    r_ref,
    k_ref,
    v_ref,
    d_ref,
    c_ref,
    g_ref,
    mix_ref,
    dcf_ref,
    gain_ref,
    bias_ref,
    w_ref,
    res_ref,
    ng_ref,
    mid_ref,
    nrm_ref,
    cut_ref,
    wbuf,
    outbox,
    inbox,
    heads,
    w_send,
    w_recv,
    f_send,
    f_recv,
    s_send,
    s_recv,
    h_send,
    h_recv,
    own_sem,
    kept,
    state,
):
    me, t = lax.axis_index("sp"), lax.axis_index("tp")
    tokens, width = r_ref.shape
    pair = 2 * CHANNEL_SPAN
    pairs = width // pair
    partner = t + 1 - 2 * lax.rem(t, 2)
    barrier = pltpu.get_barrier_semaphore()

    def greet_sp(i, carry):
        pl.semaphore_signal(
            barrier, inc=1, device_id={"sp": lax.rem(me + i, n_sp)}, device_id_type=MESH
        )
        return carry

    lax.fori_loop(1, n_sp, greet_sp, 0)
    for i in range(1, n_tp):
        pl.semaphore_signal(
            barrier, inc=1, device_id={"tp": lax.rem(t + i, n_tp)}, device_id_type=MESH
        )
    pl.semaphore_wait(barrier, n_sp - 1 + n_tp - 1)

    own = pltpu.make_async_copy(w_ref, wbuf.at[t], own_sem)
    own.start()
    w_copies = []
    for j in range(n_tp // 2):
        dest = partner if j == 0 else lax.rem(t + 2 * j, n_tp)
        copy = pltpu.make_async_remote_copy(
            src_ref=w_ref,
            dst_ref=wbuf.at[t],
            send_sem=w_send.at[j],
            recv_sem=w_recv.at[j],
            device_id={"tp": dest},
            device_id_type=MESH,
        )
        copy.start()
        w_copies.append(copy)

    f32 = jnp.float32
    row = lax.broadcasted_iota(jnp.int32, (tokens, tokens), 0)
    col = lax.broadcasted_iota(jnp.int32, (tokens, tokens), 1)
    strict = row > col
    inclusive = row >= col
    tri = jnp.where(inclusive, 1.0, 0.0).astype(f32)
    blk = head_ones(pair)
    ones_blk = jnp.where(blk, 1.0, 0.0).astype(f32)
    eye = jnp.where(
        lax.broadcasted_iota(jnp.int32, (pair, pair), 0)
        == lax.broadcasted_iota(jnp.int32, (pair, pair), 1),
        1.0,
        0.0,
    ).astype(f32)
    eye_tok = jnp.where(row == col, 1.0, 0.0).astype(f32)
    lane_head = lax.broadcasted_iota(jnp.int32, (1, pair), 1) // CHANNEL_SPAN
    lane_masks = [jnp.where(lane_head == h, 1.0, 0.0).astype(f32) for h in range(2)]

    for p in range(pairs):
        cols = pl.ds(p * pair, pair)
        recept = r_ref[:, cols].astype(f32)
        key = k_ref[:, cols].astype(f32)
        val = v_ref[:, cols].astype(f32)
        learning = 1.0 / (1.0 + jnp.exp(-c_ref[:, cols].astype(f32)))
        length = jnp.sqrt(dot_nn(key * key, ones_blk))
        unit = key / jnp.maximum(length, 1.0)
        mixed = key * (1.0 + (learning - 1.0) * mix_ref[:, cols])
        log_decay = -0.6065306597126334 / (1.0 + jnp.exp(-d_ref[:, cols].astype(f32)))
        cumulative = dot_nn(tri, log_decay)
        before = -jnp.exp(cumulative - log_decay) * unit
        inverse_decay = jnp.exp(-cumulative)
        erase = inverse_decay * unit * learning
        write = inverse_decay * mixed
        read = jnp.exp(cumulative) * recept
        removed = jnp.zeros((tokens, pair), f32)
        carried = jnp.zeros((tokens, pair), f32)
        pairs_re = []
        pairs_rw = []
        right = jnp.concatenate([erase, write], axis=0)
        for h in range(2):
            left = jnp.concatenate([before * lane_masks[h], read * lane_masks[h]], axis=0)
            prods = dot_nt(left, right)
            erase_pairs = jnp.where(strict, prods[:tokens, :tokens], 0.0)
            write_pairs = jnp.where(strict, prods[:tokens, tokens:], 0.0)
            pairs_re.append(jnp.where(inclusive, prods[tokens:, :tokens], 0.0))
            pairs_rw.append(jnp.where(inclusive, prods[tokens:, tokens:], 0.0))
            inverse = eye_tok + jnp.where(row // 2 == col // 2, erase_pairs, 0.0)
            block = 2
            while block < tokens:
                step = jnp.where(
                    (row // (2 * block) == col // (2 * block)) & (row // block != col // block),
                    erase_pairs,
                    0.0,
                )
                inverse = inverse + dot_nn(dot_nn(inverse, step), inverse)
                block *= 2
            rhs = jnp.concatenate([dot_nn(write_pairs, val), before], axis=1)
            solved = dot_nn(inverse, rhs)
            removed = removed + lane_masks[h] * solved[:, :pair]
            carried = carried + lane_masks[h] * solved[:, pair:]
        local_out = jnp.zeros((tokens, pair), f32)
        query = read
        both = jnp.concatenate([removed, carried], axis=1)
        for h in range(2):
            got = dot_nn(pairs_re[h], both)
            local_out = local_out + lane_masks[h] * (got[:, :pair] + dot_nn(pairs_rw[h], val))
            query = query + lane_masks[h] * got[:, pair:]
        final_decay = jnp.exp(cumulative[tokens - 1 : tokens, :])
        erase_end = final_decay * erase
        write_end = final_decay * write
        transit = jnp.where(blk, dot_nn(carried.T, erase_end), 0.0) + eye * final_decay
        contrib = jnp.where(
            blk, dot_nn(removed.T, erase_end) + dot_nn(val.T, write_end), 0.0
        )
        for at, full in ((0, transit), (1, contrib)):
            outbox[2 * p + at] = (full[:CHANNEL_SPAN] + full[CHANNEL_SPAN:]).astype(outbox.dtype)
        bonus = dot_nn(recept * mixed * dcf_ref[:, cols], ones_blk) * val
        kept[p, 0] = local_out
        kept[p, 1] = query
        kept[p, 2] = bonus
        state[p] = jnp.zeros((pair, pair), f32)

    def message(i):
        return pltpu.make_async_remote_copy(
            src_ref=outbox,
            dst_ref=inbox.at[me],
            send_sem=s_send.at[i],
            recv_sem=s_recv.at[me],
            device_id={"sp": i},
            device_id_type=MESH,
        )

    def send(i, carry):
        message(i).start()
        return carry

    lax.fori_loop(me + 1, n_sp, send, 0)

    def unpack(part):
        part = part.astype(f32)
        return jnp.concatenate([part * lane_masks[0], part * lane_masks[1]], axis=0)

    def hop(i, carry):
        pltpu.make_async_remote_copy(
            src_ref=outbox,
            dst_ref=inbox.at[i],
            send_sem=s_send.at[i],
            recv_sem=s_recv.at[i],
            device_id={"sp": i},
            device_id_type=MESH,
        ).wait_recv()
        for p in range(pairs):
            state[p] = dot_nn(state[p], unpack(inbox[i, 2 * p])) + unpack(inbox[i, 2 * p + 1])
        return carry

    lax.fori_loop(0, me, hop, 0)

    for p in range(pairs):
        cols = pl.ds(p * pair, pair)
        readout = kept[p, 0] + dot_nt(kept[p, 1], state[p])
        centred = readout - dot_nn(readout, ones_blk) * (1.0 / CHANNEL_SPAN)
        variance = dot_nn(centred * centred, ones_blk) * (1.0 / CHANNEL_SPAN)
        grouped = centred * lax.rsqrt(variance + GROUP_EPS) * gain_ref[:, cols] + bias_ref[:, cols]
        heads[t, :, cols] = ((grouped + kept[p, 2]) * g_ref[:, cols].astype(f32)).astype(jnp.bfloat16)

    h_copies = []
    for i in range(1, n_tp):
        copy = pltpu.make_async_remote_copy(
            src_ref=heads.at[t],
            dst_ref=heads.at[t],
            send_sem=h_send.at[i],
            recv_sem=h_recv.at[i],
            device_id={"tp": lax.rem(t + i, n_tp)},
            device_id_type=MESH,
        )
        copy.start()
        h_copies.append(copy)
    f_copies = []
    for j in range(1, n_tp // 2):
        w_copies[j].wait()
        source = lax.rem(t + n_tp - 2 * j, n_tp)
        copy = pltpu.make_async_remote_copy(
            src_ref=wbuf.at[source],
            dst_ref=wbuf.at[source],
            send_sem=f_send.at[j],
            recv_sem=f_recv.at[j],
            device_id={"tp": partner},
            device_id_type=MESH,
        )
        copy.start()
        f_copies.append(copy)
    own.wait()
    w_copies[0].wait()
    for copy in h_copies:
        copy.wait()
    for copy in f_copies:
        copy.wait()

    def drain(i, carry):
        message(i).wait_send()
        return carry

    lax.fori_loop(me + 1, n_sp, drain, 0)

    model = mid_ref.shape[1]
    whole = jnp.concatenate([heads[i] for i in range(n_tp)], axis=1)
    tile = min(512, model)
    square = jnp.zeros((tokens, 1), f32)
    for at in range(0, model, tile):
        wcol = jnp.concatenate([wbuf[i, :, at : at + tile] for i in range(n_tp)], axis=0)
        projected = jnp.dot(whole, wcol, preferred_element_type=f32)
        middle = (res_ref[:, at : at + tile].astype(f32) + projected).astype(jnp.bfloat16)
        mid_ref[:, at : at + tile] = middle
        wide = middle.astype(f32)
        square = square + jnp.sum(wide * wide, axis=1, keepdims=True)
    cut = model // n_tp
    for i in range(n_tp):

        @pl.when(t == i)
        def _():
            cut_ref[...] = mid_ref[:, i * cut : (i + 1) * cut]

    scale = lax.rsqrt(square * (1.0 / model) + NORM_EPS)
    for at in range(0, model, tile):
        wide = mid_ref[:, at : at + tile].astype(f32)
        nrm_ref[:, at : at + tile] = (wide * scale * ng_ref[:, at : at + tile]).astype(
            jnp.bfloat16
        )


def memory_and_norm(args):
    n_sp, n_tp = lax.axis_size("sp"), lax.axis_size("tp")
    r, k, v, d, c, g, mix, dcf, gain, bias, w, res, ng = args
    tokens, width = r.shape
    model = w.shape[1]
    pairs = width // (2 * CHANNEL_SPAN)
    dma = pltpu.SemaphoreType.DMA
    vm = pl.BlockSpec(memory_space=pltpu.VMEM)
    return pl.pallas_call(
        functools.partial(memory_kernel, n_sp, n_tp),
        out_shape=[jax.ShapeDtypeStruct((tokens, model), jnp.bfloat16)] * 2
        + [jax.ShapeDtypeStruct((tokens, model // n_tp), jnp.bfloat16)],
        in_specs=[vm] * 13,
        out_specs=[vm] * 3,
        scratch_shapes=[
            pltpu.VMEM((n_tp,) + w.shape, w.dtype),
            pltpu.VMEM((2 * pairs, CHANNEL_SPAN, 2 * CHANNEL_SPAN), STATE_TYPE),
            pltpu.VMEM((n_sp, 2 * pairs, CHANNEL_SPAN, 2 * CHANNEL_SPAN), STATE_TYPE),
            pltpu.VMEM((n_tp, tokens, width), jnp.bfloat16),
            dma((n_tp // 2,)),
            dma((n_tp // 2,)),
            dma((n_tp // 2,)),
            dma((n_tp // 2,)),
            dma((n_sp,)),
            dma((n_sp,)),
            dma((n_tp,)),
            dma((n_tp,)),
            dma,
            pltpu.VMEM((pairs, 3, tokens, 2 * CHANNEL_SPAN), jnp.float32),
            pltpu.VMEM((pairs, 2 * CHANNEL_SPAN, 2 * CHANNEL_SPAN), jnp.float32),
        ],
        compiler_params=pltpu.CompilerParams(
            collective_id=0, has_side_effects=True, vmem_limit_bytes=VMEM_LIMIT
        ),
        name="memory_and_norm",
    )(
        r, k, v, d, c, g,
        mix.reshape(1, -1), dcf.reshape(1, -1), gain.reshape(1, -1), bias.reshape(1, -1),
        w, res, ng.reshape(1, -1),
    )


def expert_apply(rows_in, gate_weight, up_weight, down_weight):
    gate_part = jnp.dot(rows_in, gate_weight, preferred_element_type=jnp.float32)
    up_part = jnp.dot(rows_in, up_weight, preferred_element_type=jnp.float32)
    hidden = (jax.nn.silu(gate_part) * up_part).astype(jnp.bfloat16)
    return jnp.dot(hidden, down_weight, preferred_element_type=jnp.float32)


def expert_kernel(
    n_sp,
    n_tp,
    cap,
    nrm_ref,
    own_ref,
    wt_ref,
    gate_hbm,
    up_hbm,
    down_hbm,
    cg_ref,
    cu_ref,
    cd_ref,
    out_ref,
    gate,
    up,
    down,
    blocks,
    tables,
    shared,
    rows_in,
    part,
    core_in,
    y_out,
    y_in,
    kept,
    x_out,
    x_in,
    z_out,
    z_in,
    w_sem,
    t_send,
    t_recv,
    az_send,
    az_recv,
    ax_send,
    ax_recv,
    ay_send,
    ay_recv,
    ac_send,
    ac_recv,
    rc_send,
    rc_recv,
    ry_send,
    ry_recv,
    rx_send,
    rx_recv,
    rz_send,
    rz_recv,
):
    f32, bf16 = jnp.float32, jnp.bfloat16
    me, t = lax.axis_index("sp"), lax.axis_index("tp")
    tokens, model = nrm_ref.shape
    groups = n_sp // 2
    fars = n_tp // 2
    strip = tokens // n_tp
    cols = model // n_tp
    core_to = t + 1 - 2 * lax.rem(t, 2)
    x_to = me + 1 - 2 * lax.rem(me, 2)
    parity = lax.rem(t, 2)

    def remote(src, dst, send, recv, device):
        return pltpu.make_async_remote_copy(
            src_ref=src,
            dst_ref=dst,
            send_sem=send,
            recv_sem=recv,
            device_id=device,
            device_id_type=MESH,
        )

    barrier = pltpu.get_barrier_semaphore()

    def greet(i, carry):
        pl.semaphore_signal(
            barrier, inc=1, device_id={"sp": lax.rem(me + i, n_sp)}, device_id_type=MESH
        )
        return carry

    lax.fori_loop(1, n_sp, greet, 0)
    for i in range(1, n_tp):
        pl.semaphore_signal(
            barrier, inc=1, device_id={"tp": lax.rem(t + i, n_tp)}, device_id_type=MESH
        )
    loads = [
        pltpu.make_async_copy(src, dst, w_sem.at[i])
        for i, (src, dst) in enumerate(((gate_hbm, gate), (up_hbm, up), (down_hbm, down)))
    ]
    for load in loads:
        load.start()
    pl.semaphore_wait(barrier, n_sp - 1 + n_tp - 1)

    def source(j):
        return lax.rem(me + n_sp - 2 * j, n_sp)

    def near(b):
        return b + 1 - 2 * lax.rem(b, 2)

    def rows(b, q):
        return blocks.at[b, pl.ds(pl.multiple_of(q * strip, strip), strip)]

    def own_rows():
        return nrm_ref.at[pl.ds(pl.multiple_of(t * strip, strip), strip)]

    def table_copy(i):
        to = lax.rem(me + i, n_sp)
        return remote(wt_ref.at[to], tables.at[me], t_send.at[i], t_recv.at[i], {"sp": to})

    def z_copy(j):
        to = lax.rem(me + 2 * j, n_sp)
        return remote(own_rows(), rows(me, t), az_send.at[j], az_recv.at[j], {"sp": to})

    for i in range(1, n_sp):
        table_copy(i).start()
    blocks[me] = nrm_ref[...]
    tables[me] = wt_ref[me]

    def x_own():
        return remote(own_rows(), rows(me, t), ax_send.at[0], ax_recv.at[0], {"sp": x_to})

    def x_copy(j):
        b = source(j)
        return remote(rows(b, t), rows(b, t), ax_send.at[j], ax_recv.at[j], {"sp": x_to})

    def tp_copies(j, side):
        b = source(j) if side == 0 else near(source(j))
        return [
            remote(
                rows(b, t),
                rows(b, t),
                ay_send.at[j, side, k],
                ay_recv.at[j, side, k],
                {"tp": lax.rem(t + 2 * k, n_tp)},
            )
            for k in range(1, fars)
        ]

    def core_copies(j, side):
        b = source(j) if side == 0 else near(source(j))
        found = []
        for k in range(fars):
            q = lax.rem(t + n_tp - 2 * k, n_tp)
            found.append(
                remote(
                    rows(b, q),
                    rows(b, q),
                    ac_send.at[j, side, k],
                    ac_recv.at[j, side, k],
                    {"tp": core_to},
                )
            )
        return found

    x_own().start()
    for j in range(1, groups):
        z_copy(j).start()

    slot_row = lax.broadcasted_iota(jnp.int32, (cap, tokens), 0).astype(f32)
    earlier = jnp.where(
        lax.broadcasted_iota(jnp.int32, (tokens, tokens), 0)
        < lax.broadcasted_iota(jnp.int32, (tokens, tokens), 1),
        1.0,
        0.0,
    ).astype(bf16)

    def rc_copy(j, m):
        q = 2 * m + (1 - parity)
        return remote(
            part.at[j, q], core_in.at[j, m], rc_send.at[j, m], rc_recv.at[j, m], {"tp": core_to}
        )

    def ry_copy(j, k):
        return remote(
            y_out.at[j, k],
            y_in.at[j, k],
            ry_send.at[j, k],
            ry_recv.at[j, k],
            {"tp": lax.rem(t + 2 * k, n_tp)},
        )

    def rx_copy(j):
        return remote(x_out.at[j], x_in.at[j], rx_send.at[j], rx_recv.at[j], {"sp": x_to})

    def rz_copy(j):
        return remote(
            z_out.at[j], z_in.at[j], rz_send.at[j], rz_recv.at[j], {"sp": source(j)}
        )

    def z_stage(j):
        @pl.when(j > 0)
        def _():
            z_copy(j).wait_recv()
            x_copy(j).start()
            for copy in tp_copies(j, 0):
                copy.start()

    def x_stage(j):
        x_copy(j).wait_recv()
        for copy in tp_copies(j, 1):
            copy.start()

    def y_stage(j):
        @pl.when(j > 0)
        def _():
            for copy in tp_copies(j, 0):
                copy.wait_recv()
            for copy in core_copies(j, 0):
                copy.start()

        for copy in tp_copies(j, 1):
            copy.wait_recv()
        for copy in core_copies(j, 1):
            copy.start()

    def common():
        hid = jnp.dot(nrm_ref[...], cg_ref[...], preferred_element_type=f32)
        hid = hid / (1.0 + jnp.exp(-hid)) * jnp.dot(
            nrm_ref[...], cu_ref[...], preferred_element_type=f32
        )
        hid = hid.astype(bf16)
        for q in range(n_tp):
            shared[q] = jnp.dot(
                hid, cd_ref[:, q * cols : (q + 1) * cols], preferred_element_type=f32
            )
        for load in loads:
            load.wait()

    def compute(j):
        pl.when(j == 1 % groups)(common)

        @pl.when(j > 0)
        def _():
            for copy in core_copies(j, 0):
                copy.wait_recv()
            table_copy(2 * j).wait_recv()

        for copy in core_copies(j, 1):
            copy.wait_recv()
        b0 = source(j)
        b1 = near(b0)
        table_copy(lax.rem(me + n_sp - b1, n_sp)).wait_recv()
        weighted = []
        for side, b in ((0, b0), (1, b1)):
            w = tables[b]
            routed = jnp.where(w > 0.0, 1.0, 0.0).astype(bf16)
            rank = jnp.dot(routed, earlier, preferred_element_type=f32)
            hit = (slot_row == rank[0:1, :]) & (w[0:1, :] > 0.0)
            pick = jnp.where(hit, 1.0, 0.0).astype(bf16)
            full = jnp.where(hit, w[0:1, :], 0.0).T
            high = full.astype(bf16)
            low = (full - high.astype(f32)).astype(bf16)
            weighted.append((high, low))
            for q in range(n_tp):
                at = slice(q * cols, (q + 1) * cols)
                rows_in[side * cap : (side + 1) * cap, at] = jnp.dot(
                    pick, blocks[b, :, at], preferred_element_type=f32
                ).astype(bf16)
        x = rows_in[...]
        g = jnp.dot(x, gate[0], preferred_element_type=f32)
        u = jnp.dot(x, up[0], preferred_element_type=f32)
        hidden = (g / (1.0 + jnp.exp(-g)) * u).astype(bf16)
        first = jnp.where(j == 0, 1.0, 0.0).astype(f32)
        for q in range(n_tp):
            answer = jnp.dot(
                hidden, down[0, :, q * cols : (q + 1) * cols], preferred_element_type=f32
            ).astype(bf16)
            for side in range(2):
                high, low = weighted[side]
                a = answer[side * cap : (side + 1) * cap]
                total = jnp.dot(high, a, preferred_element_type=f32) + jnp.dot(
                    low, a, preferred_element_type=f32
                )
                if side == 0:
                    total = total + first * shared[q]
                part[j, q, side * tokens : (side + 1) * tokens] = total.astype(bf16)
        for m in range(fars):
            rc_copy(j, m).start()

    def core_stage(j):
        for m in range(fars):
            rc_copy(j, m).wait_recv()
        for m in range(fars):
            q = 2 * m + parity
            x_out[j, m] = (
                part[j, q, tokens:].astype(f32) + core_in[j, m, tokens:].astype(f32)
            ).astype(bf16)
        rx_copy(j).start()

    def three_terms(j, q):
        m = lax.div(q, 2)
        return (
            part[j, q, :tokens].astype(f32)
            + core_in[j, m, :tokens].astype(f32)
            + x_in[j, m].astype(f32)
        )

    def x_reduce(j):
        rx_copy(j).wait_recv()
        for k in range(1, fars):
            y_out[j, k] = three_terms(j, lax.rem(t + 2 * k, n_tp)).astype(bf16)
            ry_copy(j, k).start()

    def y_reduce(j):
        total = three_terms(j, t)
        for k in range(1, fars):
            ry_copy(j, k).wait_recv()
            total = total + y_in[j, k].astype(f32)

        @pl.when(j == 0)
        def _():
            kept[...] = total

        @pl.when(j > 0)
        def _():
            z_out[j] = total.astype(bf16)
            rz_copy(j).start()

    stages = (
        (0, z_stage),
        (1, x_stage),
        (4, core_stage),
        (5, x_reduce),
        (6, y_reduce),
        (3, compute),
        (2, y_stage),
    )

    def step(s, carry):
        for lag, stage in stages:

            @pl.when((s >= lag) & (s < groups + lag))
            def _():
                stage(lax.rem(s - lag + 1, groups))

        return carry

    lax.fori_loop(0, groups + 6, step, 0)

    total = kept[...] + own_ref[...].astype(f32)
    for j in range(1, groups):
        rz_copy(j).wait_recv()
        total = total + z_in[j].astype(f32)
    out_ref[...] = total.astype(out_ref.dtype)

    for i in range(1, n_sp):
        table_copy(i).wait_send()
    x_own().wait_send()
    for j in range(groups):
        if j > 0:
            z_copy(j).wait_send()
            x_copy(j).wait_send()
            rz_copy(j).wait_send()
        for side in range(2):
            if j > 0 or side > 0:
                for copy in tp_copies(j, side) + core_copies(j, side):
                    copy.wait_send()
        for m in range(fars):
            rc_copy(j, m).wait_send()
        for k in range(1, fars):
            ry_copy(j, k).wait_send()
        rx_copy(j).wait_send()


def expert_layer(normed, own_cols, weights, gate, up, down, cgate, cup, cdown, cap):
    n_sp, n_tp = lax.axis_size("sp"), lax.axis_size("tp")
    tokens, model = normed.shape
    groups, fars, cols = n_sp // 2, n_tp // 2, model // n_tp
    bf16, f32 = jnp.bfloat16, jnp.float32
    dma = pltpu.SemaphoreType.DMA
    vm = pl.BlockSpec(memory_space=pltpu.VMEM)
    hbm = pl.BlockSpec(memory_space=pl.ANY)
    pairs = [dma((n_sp,)), dma((n_sp,)), dma((groups,)), dma((groups,)), dma((groups,)), dma((groups,))]
    pairs += [dma((groups, 2, fars))] * 4
    pairs += [dma((groups, fars))] * 4
    pairs += [dma((groups,))] * 4
    return pl.pallas_call(
        functools.partial(expert_kernel, n_sp, n_tp, cap),
        out_shape=jax.ShapeDtypeStruct((tokens, cols), bf16),
        in_specs=[vm, vm, vm, hbm, hbm, hbm, vm, vm, vm],
        out_specs=vm,
        scratch_shapes=[
            pltpu.VMEM(gate.shape, bf16),
            pltpu.VMEM(up.shape, bf16),
            pltpu.VMEM(down.shape, bf16),
            pltpu.VMEM((n_sp, tokens, model), bf16),
            pltpu.VMEM(weights.shape, f32),
            pltpu.VMEM((n_tp, tokens, cols), f32),
            pltpu.VMEM((2 * cap, model), bf16),
            pltpu.VMEM((groups, n_tp, 2 * tokens, cols), bf16),
            pltpu.VMEM((groups, fars, 2 * tokens, cols), bf16),
            pltpu.VMEM((groups, fars, tokens, cols), bf16),
            pltpu.VMEM((groups, fars, tokens, cols), bf16),
            pltpu.VMEM((tokens, cols), f32),
            pltpu.VMEM((groups, fars, tokens, cols), bf16),
            pltpu.VMEM((groups, fars, tokens, cols), bf16),
            pltpu.VMEM((groups, tokens, cols), bf16),
            pltpu.VMEM((groups, tokens, cols), bf16),
            dma((3,)),
        ]
        + pairs,
        compiler_params=pltpu.CompilerParams(
            collective_id=1, has_side_effects=True, vmem_limit_bytes=VMEM_LIMIT
        ),
        name="expert_layer",
    )(normed, own_cols, weights, gate, up, down, cgate, cup, cdown)


def per_device(
    receptance,
    key_by_head,
    value_head_rows,
    decay_preact,
    correction_preact,
    result_sigmoid_factor,
    key_rate_mixing,
    diagonal_current_factor,
    per_head_gain,
    per_head_bias,
    output_matrix,
    residual,
    expert_norm_gain,
    routes,
    chosen_expert_weight,
    routed_gate_weight,
    routed_up_weight,
    routed_down_weight,
    common_gate_weight,
    common_up_weight,
    common_down_weight,
):
    middle, normed, own_cols = memory_and_norm(
        (
            receptance,
            key_by_head,
            value_head_rows,
            decay_preact,
            correction_preact,
            result_sigmoid_factor,
            key_rate_mixing,
            diagonal_current_factor,
            per_head_gain,
            per_head_bias,
            output_matrix,
            residual,
            expert_norm_gain,
        )
    )
    tp_index = lax.axis_index("tp")
    tp_count = lax.axis_size("tp")
    sp_count = lax.axis_size("sp")
    token_count, top_count = routes.shape
    model_width = normed.shape[1]
    capacity = 3 * token_count * top_count // (2 * sp_count * tp_count)
    held = sp_count * token_count * model_width * normed.dtype.itemsize
    if sp_count % 2 == 0 and tp_count % 2 == 0 and 6 * held <= VMEM_LIMIT:
        mine = jnp.arange(sp_count, dtype=jnp.int32) * tp_count + tp_index
        named = routes.T[None, :, :] == mine[:, None, None]
        weights = jnp.sum(jnp.where(named, chosen_expert_weight.T[None, :, :], 0.0), axis=1)
        weights = jnp.broadcast_to(weights[:, None, :], (sp_count, 8, token_count))
        return expert_layer(
            normed,
            own_cols,
            weights,
            routed_gate_weight,
            routed_up_weight,
            routed_down_weight,
            common_gate_weight,
            common_up_weight,
            common_down_weight,
            capacity,
        )
    owned_routes = routes % tp_count == tp_index
    target = routes // tp_count
    places = jnp.arange(sp_count, dtype=jnp.int32)
    hit_counts = jnp.sum(
        jnp.where(owned_routes[:, :, None] & (target[:, :, None] == places[None, None, :]), 1, 0),
        axis=1,
    ).astype(jnp.int32)
    earlier = jnp.cumsum(hit_counts, axis=0) - hit_counts
    within = jnp.take_along_axis(earlier, target, axis=1)
    slot_index = target * capacity + within
    dropped = sp_count * capacity
    flat_slots = jnp.where(owned_routes, slot_index, dropped).reshape(-1)
    token_ids = jnp.broadcast_to(jnp.arange(token_count, dtype=jnp.int32)[:, None], routes.shape)
    slot_tokens = (
        jnp.full((dropped,), token_count, jnp.int32)
        .at[flat_slots]
        .set(token_ids.reshape(-1), mode="drop")
    )
    slot_weights = (
        jnp.zeros((dropped,), jnp.float32)
        .at[flat_slots]
        .set(chosen_expert_weight.reshape(-1), mode="drop")
    )
    padded = jnp.concatenate([normed, jnp.zeros((1, model_width), jnp.bfloat16)], axis=0)
    outgoing = padded[slot_tokens].reshape(sp_count, capacity, model_width)
    arrived = lax.all_to_all(outgoing, "sp", split_axis=0, concat_axis=0, tiled=True)
    source_count, item_count, feature_count = arrived.shape
    flat_rows = arrived.reshape(source_count * item_count, feature_count)
    answer = expert_apply(
        flat_rows, routed_gate_weight[0], routed_up_weight[0], routed_down_weight[0]
    ).astype(jnp.bfloat16)
    returned = lax.all_to_all(
        answer.reshape(source_count, item_count, feature_count),
        "sp",
        split_axis=0,
        concat_axis=0,
        tiled=True,
    )
    flat_back = returned.reshape(dropped, model_width)
    token_rows = jnp.arange(token_count, dtype=jnp.int32)
    combine_table = jnp.where(
        slot_tokens[None, :] == token_rows[:, None], slot_weights[None, :], 0.0
    )
    routed = jnp.dot(combine_table, flat_back.astype(jnp.float32), precision=HIGHEST)
    shared_out = expert_apply(normed, common_gate_weight, common_up_weight, common_down_weight)
    summed = lax.psum_scatter(
        (routed + shared_out).astype(jnp.bfloat16), "tp", scatter_dimension=1, tiled=True
    ).astype(jnp.float32)
    col_count = summed.shape[1]
    own_cols = lax.dynamic_slice_in_dim(middle, tp_index * col_count, col_count, 1)
    return (own_cols.astype(jnp.float32) + summed).astype(jnp.bfloat16)


def solution(mesh):
    return jax.shard_map(
        per_device,
        mesh=mesh,
        in_specs=(
            P("sp", "tp"),
            P("sp", "tp"),
            P("sp", "tp"),
            P("sp", "tp"),
            P("sp", "tp"),
            P("sp", "tp"),
            P("tp"),
            P("tp"),
            P("tp"),
            P("tp"),
            P("tp", None),
            P("sp", None),
            P(),
            P("sp", None),
            P("sp", None),
            P(("sp", "tp"), None, None),
            P(("sp", "tp"), None, None),
            P(("sp", "tp"), None, None),
            P(None, "tp"),
            P(None, "tp"),
            P("tp", None),
        ),
        out_specs=P("sp", "tp"),
        check_vma=False,
    )
```

```python
import functools

import jax
import jax.numpy as jnp
from jax import lax
from jax.experimental import pallas as pl
from jax.experimental.pallas import tpu as pltpu
from jax.sharding import PartitionSpec as P

CHANNEL_SPAN = 64


NORM_EPS = 1e-06
GROUP_EPS = 0.00064
HIGHEST = lax.Precision.HIGHEST
STATE_TYPE = jnp.bfloat16

MESH = pl.DeviceIdType.MESH
VMEM_LIMIT = 60 * 1024 * 1024


def dot_full(a, b):
    return lax.dot_general(
        a, b, (((1,), (0,)), ((), ())), precision=HIGHEST, preferred_element_type=jnp.float32
    )


def halves_of(a):
    high = a.astype(jnp.bfloat16)
    return high, (a - high.astype(jnp.float32)).astype(jnp.bfloat16)


def dot_nn(a, b):
    (ah, al), (bh, bl) = halves_of(a), halves_of(b)
    dot = functools.partial(jnp.dot, preferred_element_type=jnp.float32)
    return dot(ah, bh) + (dot(ah, bl) + dot(al, bh))


def dot_nt(a, b):
    return lax.dot_general(
        a, b, (((1,), (1,)), ((), ())), precision=HIGHEST, preferred_element_type=jnp.float32
    )


def head_ones(width):
    row = lax.broadcasted_iota(jnp.int32, (width, width), 0) // CHANNEL_SPAN
    col = lax.broadcasted_iota(jnp.int32, (width, width), 1) // CHANNEL_SPAN
    return row == col


def memory_kernel(
    n_sp,
    n_tp,
    r_ref,
    k_ref,
    v_ref,
    d_ref,
    c_ref,
    g_ref,
    mix_ref,
    dcf_ref,
    gain_ref,
    bias_ref,
    w_ref,
    res_ref,
    ng_ref,
    mid_ref,
    nrm_ref,
    cut_ref,
    wbuf,
    outbox,
    inbox,
    heads,
    w_send,
    w_recv,
    f_send,
    f_recv,
    s_send,
    s_recv,
    h_send,
    h_recv,
    own_sem,
    kept,
    state,
):
    me, t = lax.axis_index("sp"), lax.axis_index("tp")
    tokens, width = r_ref.shape
    pair = 2 * CHANNEL_SPAN
    pairs = width // pair
    partner = t + 1 - 2 * lax.rem(t, 2)
    barrier = pltpu.get_barrier_semaphore()

    def greet_sp(i, carry):
        pl.semaphore_signal(
            barrier, inc=1, device_id={"sp": lax.rem(me + i, n_sp)}, device_id_type=MESH
        )
        return carry

    lax.fori_loop(1, n_sp, greet_sp, 0)
    for i in range(1, n_tp):
        pl.semaphore_signal(
            barrier, inc=1, device_id={"tp": lax.rem(t + i, n_tp)}, device_id_type=MESH
        )
    pl.semaphore_wait(barrier, n_sp - 1 + n_tp - 1)

    own = pltpu.make_async_copy(w_ref, wbuf.at[t], own_sem)
    own.start()
    w_copies = []
    for j in range(n_tp // 2):
        dest = partner if j == 0 else lax.rem(t + 2 * j, n_tp)
        copy = pltpu.make_async_remote_copy(
            src_ref=w_ref,
            dst_ref=wbuf.at[t],
            send_sem=w_send.at[j],
            recv_sem=w_recv.at[j],
            device_id={"tp": dest},
            device_id_type=MESH,
        )
        copy.start()
        w_copies.append(copy)

    f32 = jnp.float32
    row = lax.broadcasted_iota(jnp.int32, (tokens, tokens), 0)
    col = lax.broadcasted_iota(jnp.int32, (tokens, tokens), 1)
    strict = row > col
    inclusive = row >= col
    tri = jnp.where(inclusive, 1.0, 0.0).astype(f32)
    blk = head_ones(pair)
    ones_blk = jnp.where(blk, 1.0, 0.0).astype(f32)
    eye = jnp.where(
        lax.broadcasted_iota(jnp.int32, (pair, pair), 0)
        == lax.broadcasted_iota(jnp.int32, (pair, pair), 1),
        1.0,
        0.0,
    ).astype(f32)
    eye_tok = jnp.where(row == col, 1.0, 0.0).astype(f32)
    lane_head = lax.broadcasted_iota(jnp.int32, (1, pair), 1) // CHANNEL_SPAN
    lane_masks = [jnp.where(lane_head == h, 1.0, 0.0).astype(f32) for h in range(2)]

    for p in range(pairs):
        cols = pl.ds(p * pair, pair)
        recept = r_ref[:, cols].astype(f32)
        key = k_ref[:, cols].astype(f32)
        val = v_ref[:, cols].astype(f32)
        learning = 1.0 / (1.0 + jnp.exp(-c_ref[:, cols].astype(f32)))
        length = jnp.sqrt(dot_nn(key * key, ones_blk))
        unit = key / jnp.maximum(length, 1.0)
        mixed = key * (1.0 + (learning - 1.0) * mix_ref[:, cols])
        log_decay = -0.6065306597126334 / (1.0 + jnp.exp(-d_ref[:, cols].astype(f32)))
        cumulative = dot_full(tri, log_decay)
        before = -jnp.exp(cumulative - log_decay) * unit
        inverse_decay = jnp.exp(-cumulative)
        erase = inverse_decay * unit * learning
        write = inverse_decay * mixed
        read = jnp.exp(cumulative) * recept
        removed = jnp.zeros((tokens, pair), f32)
        carried = jnp.zeros((tokens, pair), f32)
        right = jnp.concatenate([erase, write], axis=0)
        prods = [
            dot_nt(jnp.concatenate([before * mask, read * mask], axis=0), right)
            for mask in lane_masks
        ]
        erase_pairs = [jnp.where(strict, part[:tokens, :tokens], 0.0) for part in prods]
        write_pairs = [jnp.where(strict, part[:tokens, tokens:], 0.0) for part in prods]
        pairs_re = [jnp.where(inclusive, part[tokens:, :tokens], 0.0) for part in prods]
        pairs_rw = [jnp.where(inclusive, part[tokens:, tokens:], 0.0) for part in prods]
        inverse = [eye_tok + jnp.where(row // 2 == col // 2, part, 0.0) for part in erase_pairs]
        block = 2
        while block < tokens:
            keep = (row // (2 * block) == col // (2 * block)) & (row // block != col // block)
            halves = [
                dot_nn(inverse[h], jnp.where(keep, erase_pairs[h], 0.0)) for h in range(2)
            ]
            inverse = [inverse[h] + dot_nn(halves[h], inverse[h]) for h in range(2)]
            block *= 2
        rhs = [jnp.concatenate([dot_nn(part, val), before], axis=1) for part in write_pairs]
        solved = [dot_nn(inverse[h], rhs[h]) for h in range(2)]
        for h in range(2):
            removed = removed + lane_masks[h] * solved[h][:, :pair]
            carried = carried + lane_masks[h] * solved[h][:, pair:]
        local_out = jnp.zeros((tokens, pair), f32)
        query = read
        both = jnp.concatenate([removed, carried], axis=1)
        for h in range(2):
            got = dot_nn(pairs_re[h], both)
            local_out = local_out + lane_masks[h] * (got[:, :pair] + dot_nn(pairs_rw[h], val))
            query = query + lane_masks[h] * got[:, pair:]
        final_decay = jnp.exp(cumulative[tokens - 1 : tokens, :])
        erase_end = final_decay * erase
        write_end = final_decay * write
        transit = jnp.where(blk, dot_nn(carried.T, erase_end), 0.0) + eye * final_decay
        contrib = jnp.where(
            blk, dot_nn(removed.T, erase_end) + dot_nn(val.T, write_end), 0.0
        )
        for at, full in ((0, transit), (1, contrib)):
            outbox[2 * p + at] = (full[:CHANNEL_SPAN] + full[CHANNEL_SPAN:]).astype(outbox.dtype)
        bonus = dot_nn(recept * mixed * dcf_ref[:, cols], ones_blk) * val
        kept[p, 0] = local_out
        kept[p, 1] = query
        kept[p, 2] = bonus
        state[p] = jnp.zeros((pair, pair), f32)

    def message(i):
        return pltpu.make_async_remote_copy(
            src_ref=outbox,
            dst_ref=inbox.at[me],
            send_sem=s_send.at[i],
            recv_sem=s_recv.at[me],
            device_id={"sp": i},
            device_id_type=MESH,
        )

    def send(i, carry):
        message(i).start()
        return carry

    lax.fori_loop(me + 1, n_sp, send, 0)

    def unpack(part):
        part = part.astype(f32)
        return jnp.concatenate([part * lane_masks[0], part * lane_masks[1]], axis=0)

    def hop(i, carry):
        pltpu.make_async_remote_copy(
            src_ref=outbox,
            dst_ref=inbox.at[i],
            send_sem=s_send.at[i],
            recv_sem=s_recv.at[i],
            device_id={"sp": i},
            device_id_type=MESH,
        ).wait_recv()
        for p in range(pairs):
            state[p] = dot_nn(state[p], unpack(inbox[i, 2 * p])) + unpack(inbox[i, 2 * p + 1])
        return carry

    lax.fori_loop(0, me, hop, 0)

    for p in range(pairs):
        cols = pl.ds(p * pair, pair)
        readout = kept[p, 0] + dot_nt(kept[p, 1], state[p])
        centred = readout - dot_nn(readout, ones_blk) * (1.0 / CHANNEL_SPAN)
        variance = dot_nn(centred * centred, ones_blk) * (1.0 / CHANNEL_SPAN)
        grouped = centred * lax.rsqrt(variance + GROUP_EPS) * gain_ref[:, cols] + bias_ref[:, cols]
        heads[t, :, cols] = ((grouped + kept[p, 2]) * g_ref[:, cols].astype(f32)).astype(jnp.bfloat16)

    h_copies = []
    for i in range(1, n_tp):
        copy = pltpu.make_async_remote_copy(
            src_ref=heads.at[t],
            dst_ref=heads.at[t],
            send_sem=h_send.at[i],
            recv_sem=h_recv.at[i],
            device_id={"tp": lax.rem(t + i, n_tp)},
            device_id_type=MESH,
        )
        copy.start()
        h_copies.append(copy)
    f_copies = []
    for j in range(1, n_tp // 2):
        w_copies[j].wait()
        source = lax.rem(t + n_tp - 2 * j, n_tp)
        copy = pltpu.make_async_remote_copy(
            src_ref=wbuf.at[source],
            dst_ref=wbuf.at[source],
            send_sem=f_send.at[j],
            recv_sem=f_recv.at[j],
            device_id={"tp": partner},
            device_id_type=MESH,
        )
        copy.start()
        f_copies.append(copy)
    own.wait()
    w_copies[0].wait()
    for copy in h_copies:
        copy.wait()
    for copy in f_copies:
        copy.wait()

    def drain(i, carry):
        message(i).wait_send()
        return carry

    lax.fori_loop(me + 1, n_sp, drain, 0)

    model = mid_ref.shape[1]
    whole = jnp.concatenate([heads[i] for i in range(n_tp)], axis=1)
    tile = min(512, model)
    square = jnp.zeros((tokens, 1), f32)
    for at in range(0, model, tile):
        wcol = jnp.concatenate([wbuf[i, :, at : at + tile] for i in range(n_tp)], axis=0)
        projected = jnp.dot(whole, wcol, preferred_element_type=f32)
        middle = (res_ref[:, at : at + tile].astype(f32) + projected).astype(jnp.bfloat16)
        mid_ref[:, at : at + tile] = middle
        wide = middle.astype(f32)
        square = square + jnp.sum(wide * wide, axis=1, keepdims=True)
    cut = model // n_tp
    for i in range(n_tp):

        @pl.when(t == i)
        def _():
            cut_ref[...] = mid_ref[:, i * cut : (i + 1) * cut]

    scale = lax.rsqrt(square * (1.0 / model) + NORM_EPS)
    for at in range(0, model, tile):
        wide = mid_ref[:, at : at + tile].astype(f32)
        nrm_ref[:, at : at + tile] = (wide * scale * ng_ref[:, at : at + tile]).astype(
            jnp.bfloat16
        )


def memory_and_norm(args):
    n_sp, n_tp = lax.axis_size("sp"), lax.axis_size("tp")
    r, k, v, d, c, g, mix, dcf, gain, bias, w, res, ng = args
    tokens, width = r.shape
    model = w.shape[1]
    pairs = width // (2 * CHANNEL_SPAN)
    dma = pltpu.SemaphoreType.DMA
    vm = pl.BlockSpec(memory_space=pltpu.VMEM)
    return pl.pallas_call(
        functools.partial(memory_kernel, n_sp, n_tp),
        out_shape=[jax.ShapeDtypeStruct((tokens, model), jnp.bfloat16)] * 2
        + [jax.ShapeDtypeStruct((tokens, model // n_tp), jnp.bfloat16)],
        in_specs=[vm] * 13,
        out_specs=[vm] * 3,
        scratch_shapes=[
            pltpu.VMEM((n_tp,) + w.shape, w.dtype),
            pltpu.VMEM((2 * pairs, CHANNEL_SPAN, 2 * CHANNEL_SPAN), STATE_TYPE),
            pltpu.VMEM((n_sp, 2 * pairs, CHANNEL_SPAN, 2 * CHANNEL_SPAN), STATE_TYPE),
            pltpu.VMEM((n_tp, tokens, width), jnp.bfloat16),
            dma((n_tp // 2,)),
            dma((n_tp // 2,)),
            dma((n_tp // 2,)),
            dma((n_tp // 2,)),
            dma((n_sp,)),
            dma((n_sp,)),
            dma((n_tp,)),
            dma((n_tp,)),
            dma,
            pltpu.VMEM((pairs, 3, tokens, 2 * CHANNEL_SPAN), jnp.float32),
            pltpu.VMEM((pairs, 2 * CHANNEL_SPAN, 2 * CHANNEL_SPAN), jnp.float32),
        ],
        compiler_params=pltpu.CompilerParams(
            collective_id=0, has_side_effects=True, vmem_limit_bytes=VMEM_LIMIT
        ),
        name="memory_and_norm",
    )(
        r, k, v, d, c, g,
        mix.reshape(1, -1), dcf.reshape(1, -1), gain.reshape(1, -1), bias.reshape(1, -1),
        w, res, ng.reshape(1, -1),
    )


def expert_apply(rows_in, gate_weight, up_weight, down_weight):
    gate_part = jnp.dot(rows_in, gate_weight, preferred_element_type=jnp.float32)
    up_part = jnp.dot(rows_in, up_weight, preferred_element_type=jnp.float32)
    hidden = (jax.nn.silu(gate_part) * up_part).astype(jnp.bfloat16)
    return jnp.dot(hidden, down_weight, preferred_element_type=jnp.float32)


def expert_kernel(
    n_sp,
    n_tp,
    cap,
    nrm_ref,
    own_ref,
    wt_ref,
    gate_hbm,
    up_hbm,
    down_hbm,
    cg_ref,
    cu_ref,
    cd_ref,
    out_ref,
    gate,
    up,
    down,
    blocks,
    tables,
    shared,
    rows_in,
    part,
    core_in,
    y_out,
    y_in,
    kept,
    x_out,
    x_in,
    z_out,
    z_in,
    w_sem,
    t_send,
    t_recv,
    az_send,
    az_recv,
    ax_send,
    ax_recv,
    ay_send,
    ay_recv,
    ac_send,
    ac_recv,
    rc_send,
    rc_recv,
    ry_send,
    ry_recv,
    rx_send,
    rx_recv,
    rz_send,
    rz_recv,
):
    f32, bf16 = jnp.float32, jnp.bfloat16
    me, t = lax.axis_index("sp"), lax.axis_index("tp")
    tokens, model = nrm_ref.shape
    groups = n_sp // 2
    fars = n_tp // 2
    strip = tokens // n_tp
    cols = model // n_tp
    core_to = t + 1 - 2 * lax.rem(t, 2)
    x_to = me + 1 - 2 * lax.rem(me, 2)
    parity = lax.rem(t, 2)

    def remote(src, dst, send, recv, device):
        return pltpu.make_async_remote_copy(
            src_ref=src,
            dst_ref=dst,
            send_sem=send,
            recv_sem=recv,
            device_id=device,
            device_id_type=MESH,
        )

    barrier = pltpu.get_barrier_semaphore()

    def greet(i, carry):
        pl.semaphore_signal(
            barrier, inc=1, device_id={"sp": lax.rem(me + i, n_sp)}, device_id_type=MESH
        )
        return carry

    lax.fori_loop(1, n_sp, greet, 0)
    for i in range(1, n_tp):
        pl.semaphore_signal(
            barrier, inc=1, device_id={"tp": lax.rem(t + i, n_tp)}, device_id_type=MESH
        )
    loads = [
        pltpu.make_async_copy(src, dst, w_sem.at[i])
        for i, (src, dst) in enumerate(((gate_hbm, gate), (up_hbm, up), (down_hbm, down)))
    ]
    for load in loads:
        load.start()
    pl.semaphore_wait(barrier, n_sp - 1 + n_tp - 1)

    def source(j):
        return lax.rem(me + n_sp - 2 * j, n_sp)

    def near(b):
        return b + 1 - 2 * lax.rem(b, 2)

    def rows(b, q):
        return blocks.at[b, pl.ds(pl.multiple_of(q * strip, strip), strip)]

    def own_rows():
        return nrm_ref.at[pl.ds(pl.multiple_of(t * strip, strip), strip)]

    def table_copy(i):
        to = lax.rem(me + i, n_sp)
        return remote(wt_ref.at[to], tables.at[me], t_send.at[i], t_recv.at[i], {"sp": to})

    def z_copy(j):
        to = lax.rem(me + 2 * j, n_sp)
        return remote(own_rows(), rows(me, t), az_send.at[j], az_recv.at[j], {"sp": to})

    for i in range(1, n_sp):
        table_copy(i).start()
    blocks[me] = nrm_ref[...]
    tables[me] = wt_ref[me]

    def x_own():
        return remote(own_rows(), rows(me, t), ax_send.at[0], ax_recv.at[0], {"sp": x_to})

    def x_copy(j):
        b = source(j)
        return remote(rows(b, t), rows(b, t), ax_send.at[j], ax_recv.at[j], {"sp": x_to})

    def tp_copies(j, side):
        b = source(j) if side == 0 else near(source(j))
        return [
            remote(
                rows(b, t),
                rows(b, t),
                ay_send.at[j, side, k],
                ay_recv.at[j, side, k],
                {"tp": lax.rem(t + 2 * k, n_tp)},
            )
            for k in range(1, fars)
        ]

    def core_copies(j, side):
        b = source(j) if side == 0 else near(source(j))
        found = []
        for k in range(fars):
            q = lax.rem(t + n_tp - 2 * k, n_tp)
            found.append(
                remote(
                    rows(b, q),
                    rows(b, q),
                    ac_send.at[j, side, k],
                    ac_recv.at[j, side, k],
                    {"tp": core_to},
                )
            )
        return found

    x_own().start()
    for j in range(1, groups):
        z_copy(j).start()

    slot_row = lax.broadcasted_iota(jnp.int32, (cap, tokens), 0).astype(f32)
    earlier = jnp.where(
        lax.broadcasted_iota(jnp.int32, (tokens, tokens), 0)
        < lax.broadcasted_iota(jnp.int32, (tokens, tokens), 1),
        1.0,
        0.0,
    ).astype(bf16)

    def rc_copy(j, m):
        q = 2 * m + (1 - parity)
        return remote(
            part.at[j, q], core_in.at[j, m], rc_send.at[j, m], rc_recv.at[j, m], {"tp": core_to}
        )

    def ry_copy(j, k):
        return remote(
            y_out.at[j, k],
            y_in.at[j, k],
            ry_send.at[j, k],
            ry_recv.at[j, k],
            {"tp": lax.rem(t + 2 * k, n_tp)},
        )

    def rx_copy(j):
        return remote(x_out.at[j], x_in.at[j], rx_send.at[j], rx_recv.at[j], {"sp": x_to})

    def rz_copy(j):
        return remote(
            z_out.at[j], z_in.at[j], rz_send.at[j], rz_recv.at[j], {"sp": source(j)}
        )

    def z_stage(j):
        @pl.when(j > 0)
        def _():
            z_copy(j).wait_recv()
            x_copy(j).start()
            for copy in tp_copies(j, 0):
                copy.start()

    def x_stage(j):
        x_copy(j).wait_recv()
        for copy in tp_copies(j, 1):
            copy.start()

    def y_stage(j):
        @pl.when(j > 0)
        def _():
            for copy in tp_copies(j, 0):
                copy.wait_recv()
            for copy in core_copies(j, 0):
                copy.start()

        for copy in tp_copies(j, 1):
            copy.wait_recv()
        for copy in core_copies(j, 1):
            copy.start()

    def common():
        hid = jnp.dot(nrm_ref[...], cg_ref[...], preferred_element_type=f32)
        hid = hid / (1.0 + jnp.exp(-hid)) * jnp.dot(
            nrm_ref[...], cu_ref[...], preferred_element_type=f32
        )
        hid = hid.astype(bf16)
        for q in range(n_tp):
            shared[q] = jnp.dot(
                hid, cd_ref[:, q * cols : (q + 1) * cols], preferred_element_type=f32
            )
        for load in loads:
            load.wait()

    def compute(j):
        pl.when(j == 1 % groups)(common)

        @pl.when(j > 0)
        def _():
            for copy in core_copies(j, 0):
                copy.wait_recv()
            table_copy(2 * j).wait_recv()

        for copy in core_copies(j, 1):
            copy.wait_recv()
        b0 = source(j)
        b1 = near(b0)
        table_copy(lax.rem(me + n_sp - b1, n_sp)).wait_recv()
        weighted = []
        for side, b in ((0, b0), (1, b1)):
            w = tables[b]
            routed = jnp.where(w > 0.0, 1.0, 0.0).astype(bf16)
            rank = jnp.dot(routed, earlier, preferred_element_type=f32)
            hit = (slot_row == rank[0:1, :]) & (w[0:1, :] > 0.0)
            pick = jnp.where(hit, 1.0, 0.0).astype(bf16)
            full = jnp.where(hit, w[0:1, :], 0.0).T
            high = full.astype(bf16)
            low = (full - high.astype(f32)).astype(bf16)
            weighted.append((high, low))
            for q in range(n_tp):
                at = slice(q * cols, (q + 1) * cols)
                rows_in[side * cap : (side + 1) * cap, at] = jnp.dot(
                    pick, blocks[b, :, at], preferred_element_type=f32
                ).astype(bf16)
        x = rows_in[...]
        g = jnp.dot(x, gate[0], preferred_element_type=f32)
        u = jnp.dot(x, up[0], preferred_element_type=f32)
        hidden = (g / (1.0 + jnp.exp(-g)) * u).astype(bf16)
        first = jnp.where(j == 0, 1.0, 0.0).astype(f32)
        for q in range(n_tp):
            answer = jnp.dot(
                hidden, down[0, :, q * cols : (q + 1) * cols], preferred_element_type=f32
            ).astype(bf16)
            for side in range(2):
                high, low = weighted[side]
                a = answer[side * cap : (side + 1) * cap]
                total = jnp.dot(high, a, preferred_element_type=f32) + jnp.dot(
                    low, a, preferred_element_type=f32
                )
                if side == 0:
                    total = total + first * shared[q]
                part[j, q, side * tokens : (side + 1) * tokens] = total.astype(bf16)
        for m in range(fars):
            rc_copy(j, m).start()

    def core_stage(j):
        for m in range(fars):
            rc_copy(j, m).wait_recv()
        for m in range(fars):
            q = 2 * m + parity
            x_out[j, m] = (
                part[j, q, tokens:].astype(f32) + core_in[j, m, tokens:].astype(f32)
            ).astype(bf16)
        rx_copy(j).start()

    def three_terms(j, q):
        m = lax.div(q, 2)
        return (
            part[j, q, :tokens].astype(f32)
            + core_in[j, m, :tokens].astype(f32)
            + x_in[j, m].astype(f32)
        )

    def x_reduce(j):
        rx_copy(j).wait_recv()
        for k in range(1, fars):
            y_out[j, k] = three_terms(j, lax.rem(t + 2 * k, n_tp)).astype(bf16)
            ry_copy(j, k).start()

    def y_reduce(j):
        total = three_terms(j, t)
        for k in range(1, fars):
            ry_copy(j, k).wait_recv()
            total = total + y_in[j, k].astype(f32)

        @pl.when(j == 0)
        def _():
            kept[...] = total

        @pl.when(j > 0)
        def _():
            z_out[j] = total.astype(bf16)
            rz_copy(j).start()

    stages = (
        (0, z_stage),
        (1, x_stage),
        (4, core_stage),
        (5, x_reduce),
        (6, y_reduce),
        (3, compute),
        (2, y_stage),
    )

    def step(s, carry):
        for lag, stage in stages:

            @pl.when((s >= lag) & (s < groups + lag))
            def _():
                stage(lax.rem(s - lag + 1, groups))

        return carry

    lax.fori_loop(0, groups + 6, step, 0)

    total = kept[...] + own_ref[...].astype(f32)
    for j in range(1, groups):
        rz_copy(j).wait_recv()
        total = total + z_in[j].astype(f32)
    out_ref[...] = total.astype(out_ref.dtype)

    for i in range(1, n_sp):
        table_copy(i).wait_send()
    x_own().wait_send()
    for j in range(groups):
        if j > 0:
            z_copy(j).wait_send()
            x_copy(j).wait_send()
            rz_copy(j).wait_send()
        for side in range(2):
            if j > 0 or side > 0:
                for copy in tp_copies(j, side) + core_copies(j, side):
                    copy.wait_send()
        for m in range(fars):
            rc_copy(j, m).wait_send()
        for k in range(1, fars):
            ry_copy(j, k).wait_send()
        rx_copy(j).wait_send()


def expert_layer(normed, own_cols, weights, gate, up, down, cgate, cup, cdown, cap):
    n_sp, n_tp = lax.axis_size("sp"), lax.axis_size("tp")
    tokens, model = normed.shape
    groups, fars, cols = n_sp // 2, n_tp // 2, model // n_tp
    bf16, f32 = jnp.bfloat16, jnp.float32
    dma = pltpu.SemaphoreType.DMA
    vm = pl.BlockSpec(memory_space=pltpu.VMEM)
    hbm = pl.BlockSpec(memory_space=pl.ANY)
    pairs = [dma((n_sp,)), dma((n_sp,)), dma((groups,)), dma((groups,)), dma((groups,)), dma((groups,))]
    pairs += [dma((groups, 2, fars))] * 4
    pairs += [dma((groups, fars))] * 4
    pairs += [dma((groups,))] * 4
    return pl.pallas_call(
        functools.partial(expert_kernel, n_sp, n_tp, cap),
        out_shape=jax.ShapeDtypeStruct((tokens, cols), bf16),
        in_specs=[vm, vm, vm, hbm, hbm, hbm, vm, vm, vm],
        out_specs=vm,
        scratch_shapes=[
            pltpu.VMEM(gate.shape, bf16),
            pltpu.VMEM(up.shape, bf16),
            pltpu.VMEM(down.shape, bf16),
            pltpu.VMEM((n_sp, tokens, model), bf16),
            pltpu.VMEM(weights.shape, f32),
            pltpu.VMEM((n_tp, tokens, cols), f32),
            pltpu.VMEM((2 * cap, model), bf16),
            pltpu.VMEM((groups, n_tp, 2 * tokens, cols), bf16),
            pltpu.VMEM((groups, fars, 2 * tokens, cols), bf16),
            pltpu.VMEM((groups, fars, tokens, cols), bf16),
            pltpu.VMEM((groups, fars, tokens, cols), bf16),
            pltpu.VMEM((tokens, cols), f32),
            pltpu.VMEM((groups, fars, tokens, cols), bf16),
            pltpu.VMEM((groups, fars, tokens, cols), bf16),
            pltpu.VMEM((groups, tokens, cols), bf16),
            pltpu.VMEM((groups, tokens, cols), bf16),
            dma((3,)),
        ]
        + pairs,
        compiler_params=pltpu.CompilerParams(
            collective_id=1, has_side_effects=True, vmem_limit_bytes=VMEM_LIMIT
        ),
        name="expert_layer",
    )(normed, own_cols, weights, gate, up, down, cgate, cup, cdown)


def per_device(
    receptance,
    key_by_head,
    value_head_rows,
    decay_preact,
    correction_preact,
    result_sigmoid_factor,
    key_rate_mixing,
    diagonal_current_factor,
    per_head_gain,
    per_head_bias,
    output_matrix,
    residual,
    expert_norm_gain,
    routes,
    chosen_expert_weight,
    routed_gate_weight,
    routed_up_weight,
    routed_down_weight,
    common_gate_weight,
    common_up_weight,
    common_down_weight,
):
    middle, normed, own_cols = memory_and_norm(
        (
            receptance,
            key_by_head,
            value_head_rows,
            decay_preact,
            correction_preact,
            result_sigmoid_factor,
            key_rate_mixing,
            diagonal_current_factor,
            per_head_gain,
            per_head_bias,
            output_matrix,
            residual,
            expert_norm_gain,
        )
    )
    tp_index = lax.axis_index("tp")
    tp_count = lax.axis_size("tp")
    sp_count = lax.axis_size("sp")
    token_count, top_count = routes.shape
    model_width = normed.shape[1]
    capacity = 3 * token_count * top_count // (2 * sp_count * tp_count)
    held = sp_count * token_count * model_width * normed.dtype.itemsize
    if sp_count % 2 == 0 and tp_count % 2 == 0 and 6 * held <= VMEM_LIMIT:
        mine = jnp.arange(sp_count, dtype=jnp.int32) * tp_count + tp_index
        named = routes.T[None, :, :] == mine[:, None, None]
        weights = jnp.sum(jnp.where(named, chosen_expert_weight.T[None, :, :], 0.0), axis=1)
        weights = jnp.broadcast_to(weights[:, None, :], (sp_count, 8, token_count))
        return expert_layer(
            normed,
            own_cols,
            weights,
            routed_gate_weight,
            routed_up_weight,
            routed_down_weight,
            common_gate_weight,
            common_up_weight,
            common_down_weight,
            capacity,
        )
    owned_routes = routes % tp_count == tp_index
    target = routes // tp_count
    places = jnp.arange(sp_count, dtype=jnp.int32)
    hit_counts = jnp.sum(
        jnp.where(owned_routes[:, :, None] & (target[:, :, None] == places[None, None, :]), 1, 0),
        axis=1,
    ).astype(jnp.int32)
    earlier = jnp.cumsum(hit_counts, axis=0) - hit_counts
    within = jnp.take_along_axis(earlier, target, axis=1)
    slot_index = target * capacity + within
    dropped = sp_count * capacity
    flat_slots = jnp.where(owned_routes, slot_index, dropped).reshape(-1)
    token_ids = jnp.broadcast_to(jnp.arange(token_count, dtype=jnp.int32)[:, None], routes.shape)
    slot_tokens = (
        jnp.full((dropped,), token_count, jnp.int32)
        .at[flat_slots]
        .set(token_ids.reshape(-1), mode="drop")
    )
    slot_weights = (
        jnp.zeros((dropped,), jnp.float32)
        .at[flat_slots]
        .set(chosen_expert_weight.reshape(-1), mode="drop")
    )
    padded = jnp.concatenate([normed, jnp.zeros((1, model_width), jnp.bfloat16)], axis=0)
    outgoing = padded[slot_tokens].reshape(sp_count, capacity, model_width)
    arrived = lax.all_to_all(outgoing, "sp", split_axis=0, concat_axis=0, tiled=True)
    source_count, item_count, feature_count = arrived.shape
    flat_rows = arrived.reshape(source_count * item_count, feature_count)
    answer = expert_apply(
        flat_rows, routed_gate_weight[0], routed_up_weight[0], routed_down_weight[0]
    ).astype(jnp.bfloat16)
    returned = lax.all_to_all(
        answer.reshape(source_count, item_count, feature_count),
        "sp",
        split_axis=0,
        concat_axis=0,
        tiled=True,
    )
    flat_back = returned.reshape(dropped, model_width)
    token_rows = jnp.arange(token_count, dtype=jnp.int32)
    combine_table = jnp.where(
        slot_tokens[None, :] == token_rows[:, None], slot_weights[None, :], 0.0
    )
    routed = jnp.dot(combine_table, flat_back.astype(jnp.float32), precision=HIGHEST)
    shared_out = expert_apply(normed, common_gate_weight, common_up_weight, common_down_weight)
    summed = lax.psum_scatter(
        (routed + shared_out).astype(jnp.bfloat16), "tp", scatter_dimension=1, tiled=True
    ).astype(jnp.float32)
    col_count = summed.shape[1]
    own_cols = lax.dynamic_slice_in_dim(middle, tp_index * col_count, col_count, 1)
    return (own_cols.astype(jnp.float32) + summed).astype(jnp.bfloat16)


def solution(mesh):
    return jax.shard_map(
        per_device,
        mesh=mesh,
        in_specs=(
            P("sp", "tp"),
            P("sp", "tp"),
            P("sp", "tp"),
            P("sp", "tp"),
            P("sp", "tp"),
            P("sp", "tp"),
            P("tp"),
            P("tp"),
            P("tp"),
            P("tp"),
            P("tp", None),
            P("sp", None),
            P(),
            P("sp", None),
            P("sp", None),
            P(("sp", "tp"), None, None),
            P(("sp", "tp"), None, None),
            P(("sp", "tp"), None, None),
            P(None, "tp"),
            P(None, "tp"),
            P("tp", None),
        ),
        out_specs=P("sp", "tp"),
        check_vma=False,
    )
```
